32 devices in a mesh: ep: 8 (over z, y), tp: 4 (over x, core).
Axes of the slice: x: 2, y: 2, z: 4, core: 2. Of those that a mesh axis runs over, the one named last changes fastest.
Arguments:
- tokens: bfloat16 [192, 1024], P('ep'), may hold values from -6 to 6
- mixer_gain: float32 [1024], replicated, may hold values from 0.1 to 1.9
- gate_weight: bfloat16 [1024, 1024], P(None, 'tp'), may hold values from -0.1875 to 0.1875
- inner_weight: bfloat16 [1024, 1024], P(None, 'tp'), may hold values from -0.1875 to 0.1875
- state_weight: bfloat16 [2, 1024, 512], P(None, None, 'tp'), may hold values from -0.1875 to 0.1875
- step_weight: bfloat16 [1024, 16], P(None, 'tp'), may hold values from -0.1875 to 0.1875
- step_bias: float32 [16], P('tp'), may hold values from -4 to 0.5
- decay_log: float32 [16], P('tp'), may hold values from 0 to 2.8
- skip_scale: float32 [16], P('tp'), may hold values from 0.5 to 1.5
- inner_kernel: float32 [4, 1024], P(None, 'tp'), may hold values from -3 to 3
- state_kernel: float32 [4, 2, 512], P(None, None, 'tp'), may hold values from -3 to 3
- inner_window: bfloat16 [192, 3, 1024], P('ep', None, 'tp'), may hold values from -6 to 6
- state_window: bfloat16 [192, 3, 2, 512], P('ep', None, None, 'tp'), may hold values from -6 to 6
- recurrent_state: float32 [192, 16, 64, 128], P('ep', 'tp'), may hold values from -2.4 to 2.4
- group_gain: float32 [1024], P('tp'), may hold values from 0.1 to 1.9
- output_weight: bfloat16 [1024, 1024], P('tp'), may hold values from -0.1875 to 0.1875
- channel_gain: float32 [1024], replicated, may hold values from 0.1 to 1.9
- routes: int32 [192, 2], P('ep'), may hold values from 0 to 7, all different within a row; in each aligned block of 24 rows (0 to 23, 24 to 47, ...) at most 9 rows name the same one
- route_weights: float32 [192, 2], P('ep'), may hold values from 0.2 to 1
- expert_gate: bfloat16 [8, 1024, 2816], P('ep', None, 'tp'), may hold values from -0.1875 to 0.1875
- expert_up: bfloat16 [8, 1024, 2816], P('ep', None, 'tp'), may hold values from -0.1875 to 0.1875
- expert_down: bfloat16 [8, 2816, 1024], P('ep', 'tp'), may hold values from -0.109375 to 0.109375
- dense_gate: bfloat16 [1024, 2816], P('tp', 'ep'), may hold values from -0.1875 to 0.1875
- dense_up: bfloat16 [1024, 2816], P('tp', 'ep'), may hold values from -0.1875 to 0.1875
- dense_down: bfloat16 [2816, 1024], P('ep', 'tp'), may hold values from -0.109375 to 0.109375
- dense_scale: float32 [1024], P('tp'), may hold values from 0.3 to 1.5
Outputs:
- new_tokens: bfloat16 [192, 1024], P('ep', 'tp')
- new_state: float32 [192, 16, 64, 128], P('ep', 'tp')
- new_inner_window: bfloat16 [192, 3, 1024], P('ep', None, 'tp')
- new_state_window: bfloat16 [192, 3, 2, 512], P('ep', None, None, 'tp')
The draws below stay inside these ranges and needn't reach their ends.
Inputs may be any that keep to these rules, and one draw needn't show every extreme that they name: `routes`: each row names 2 different experts. Within the rows of one device (aligned blocks of 24 rows) no expert is named by more than 9 rows, and in some block an expert is named by exactly 9 rows.
All inputs are finite; a program needn't handle non-finite values.
Results may differ from the reference program's by a relative error of at most 0.014.
Values may be sent and summed in bfloat16 or wider, within the bound.
A program may use at most 64 MiB of HBM per device.

```python
import math
import jax
import jax.numpy as jnp
import numpy as np
from jax import lax

D = 1024
HEADS = 16
GROUPS = 4
HEAD_DIM = 64
STATE_DIM = 128
CONV = 4
FF = 2816
FFD = 2816
TOPK = 2
S_DEV = 24
EXPERTS = 8
BATCH = 192
INNER = 1024
BC = 512
CAP = 9
N_EP = 8
N_TP = 4


def steps_of(own_key, dims, pieces, low, high):
    loudness, own = 1.0, jax.random.fold_in(own_key, 6)
    for axis_at, parts in pieces:
        draws = jnp.exp(jax.random.uniform(jax.random.fold_in(own, axis_at), (parts,), jnp.float32, low / len(pieces), high / len(pieces)))
        loudness = loudness * jnp.repeat(draws, dims[axis_at] // parts).reshape([-1 if axis == axis_at else 1 for axis in range(len(dims))])
    return loudness


def deal_out(own_key, own, number, rows, amount, top, bound, slope):
    order = jax.random.permutation(own_key, amount)
    crowded, ordinary = shares(amount, rows * top, bound, slope, True), shares(amount, rows * top, bound, slope, False)
    places = jnp.arange(amount)

    def named(sizes, offset_by):
        used = int((sizes > 0).sum())
        fixed = max(1, used // 4)
        shifted = fixed + (places - fixed + offset_by * (used - fixed)) % max(1, amount - fixed)
        return jnp.zeros((amount,), jnp.int32).at[order[jnp.where(places < fixed, places, shifted)]].set(jnp.asarray(sizes, jnp.int32))

    sizes = jnp.where(number % 4 == 0, named(crowded, number // 4), named(ordinary, number - number // 4 - 1))
    mixed = jax.random.permutation(jax.random.fold_in(own, 3), amount)
    giver, sink = mixed[0:amount // 2 * 2:2], mixed[1:amount // 2 * 2:2]
    room = jnp.minimum(sizes[giver] - 1, bound - sizes[sink]) // 2
    room = jnp.where((giver == order[0]) | (sink == order[0]) | (sizes[sink] == 0), 0, jnp.maximum(room, 0))
    shifted = jax.random.randint(jax.random.fold_in(own, 4), (amount // 2,), 0, 1 << 20) % (room + 1)
    sizes = sizes.at[giver].add(-shifted).at[sink].add(shifted)
    items = jnp.searchsorted(jnp.cumsum(sizes), jnp.arange(rows * top), side="right").astype(jnp.int32)
    listing = items.reshape(top, rows).T
    listing = listing[jax.random.permutation(jax.random.fold_in(own, 1), rows)]
    offset_by = jax.random.randint(jax.random.fold_in(own, 2), (rows, 1), 0, top)
    return jnp.take_along_axis(listing, (jnp.arange(top)[None, :] + offset_by) % top, axis=1)


def shares(count, total, bound, skew, full):
    weights = [(1 << 20) // math.isqrt(rank ** skew) + 1 for rank in range(1, count + 1)]
    largest = bound if full else min(bound, max(-(-total // count), total * weights[0] // sum(weights)))
    least = 1 if total - largest >= count - 1 else 0
    given, spare = [largest] + [least] * (count - 1), total - largest - least * (count - 1)
    while spare > 0:
        candidates = [i for i in range(1, count) if given[i] < largest] or [i for i in range(1, count) if given[i] < bound]
        pool, left = sum([weights[i] for i in candidates]), spare
        for i in candidates:
            addition = min(bound - given[i], max(1, left * weights[i] // pool), spare)
            given[i] = given[i] + addition
            spare = spare - addition
    return np.array(given)


def noise(own_key, extent, spread, most, shards=(), kind=jnp.bfloat16):
    array = jax.random.normal(own_key, extent, jnp.float32) * spread
    if len(shards) > 0:
        array = steps_of(own_key, extent, shards, -0.22, 0.18) * array
    return jnp.clip(array, min=-most, max=most).astype(kind)


def setup_inputs(seed: int = 0) -> dict:
    arg_keys = jax.random.split(jax.random.key(seed), 27)
    tokens = noise(arg_keys[0], (BATCH, D), 1.0, 6.0, ((0, 8),))
    mixer_gain = jnp.clip(1.0 + 0.18 * jax.random.normal(arg_keys[1], (D,), jnp.float32), 0.1, 1.9)
    gate_weight = noise(arg_keys[2], (D, INNER), D ** -0.5, 0.1875, ((1, 4),))
    inner_weight = noise(arg_keys[3], (D, INNER), D ** -0.5, 0.1875, ((1, 4),))
    state_weight = noise(arg_keys[4], (2, D, BC), D ** -0.5, 0.1875, ((2, 4),))
    step_weight = noise(arg_keys[5], (D, HEADS), D ** -0.5, 0.1875, ((1, 4),))
    step_bias = jnp.clip(-4.0 + 4.5 * jax.random.uniform(arg_keys[6], (HEADS,), jnp.float32) ** steps_of(arg_keys[6], (HEADS,), ((0, 4),), -0.2, 0.2), -4.0, 0.5)
    decay_log = jnp.clip(2.8 * jax.random.uniform(arg_keys[7], (HEADS,), jnp.float32) ** steps_of(arg_keys[7], (HEADS,), ((0, 4),), -0.2, 0.2), 0.0, 2.8)
    skip_scale = jnp.clip(0.5 + 1.0 * jax.random.uniform(arg_keys[8], (HEADS,), jnp.float32) ** steps_of(arg_keys[8], (HEADS,), ((0, 4),), -0.2, 0.2), 0.5, 1.5)
    inner_kernel = noise(arg_keys[9], (CONV, INNER), CONV ** -0.5, 3.0, ((1, 4),), jnp.float32)
    state_kernel = noise(arg_keys[10], (CONV, 2, BC), CONV ** -0.5, 3.0, ((2, 4),), jnp.float32)
    inner_window = noise(arg_keys[11], (BATCH, CONV - 1, INNER), 1.0, 6.0, ((0, 8), (2, 4)))
    state_window = noise(arg_keys[12], (BATCH, CONV - 1, 2, BC), 1.0, 6.0, ((0, 8), (3, 4)))
    recurrent_state = noise(arg_keys[13], (BATCH, HEADS, HEAD_DIM, STATE_DIM), 0.3, 2.4, ((0, 8), (1, 4)), jnp.float32)
    group_gain = jnp.clip(1.0 + 0.18 * jax.random.normal(arg_keys[14], (INNER,), jnp.float32), 0.1, 1.9)
    output_weight = noise(arg_keys[15], (INNER, D), INNER ** -0.5, 0.1875, ((0, 4),))
    channel_gain = jnp.clip(1.0 + 0.18 * jax.random.normal(arg_keys[16], (D,), jnp.float32), 0.1, 1.9)
    routes_keys = jax.random.split(jax.random.fold_in(arg_keys[17], 1), BATCH // S_DEV)
    routes_turns = jax.random.permutation(jax.random.fold_in(arg_keys[17], 3), BATCH // S_DEV)
    routes = jax.vmap(lambda own, number: deal_out(jax.random.fold_in(arg_keys[17], 2), own, number, S_DEV, EXPERTS, TOPK, CAP, 2))(routes_keys, routes_turns).reshape((BATCH, TOPK))
    route_weights = jnp.clip(0.2 + 0.8 * jax.random.uniform(arg_keys[18], (BATCH, TOPK), jnp.float32) ** steps_of(arg_keys[18], (BATCH, TOPK), ((0, 8),), -0.2, 0.2), 0.2, 1.0)
    expert_gate = noise(arg_keys[19], (EXPERTS, D, FF), D ** -0.5, 0.1875, ((0, 8), (2, 4)))
    expert_up = noise(arg_keys[20], (EXPERTS, D, FF), D ** -0.5, 0.1875, ((0, 8), (2, 4)))
    expert_down = noise(arg_keys[21], (EXPERTS, FF, D), FF ** -0.5, 0.109375, ((0, 8), (1, 4)))
    dense_gate = noise(arg_keys[22], (D, FFD), D ** -0.5, 0.1875, ((0, 4), (1, 8)))
    dense_up = noise(arg_keys[23], (D, FFD), D ** -0.5, 0.1875, ((0, 4), (1, 8)))
    dense_down = noise(arg_keys[24], (FFD, D), FFD ** -0.5, 0.109375, ((0, 8), (1, 4)))
    dense_scale = jnp.clip(0.3 + 1.2 * jax.random.uniform(arg_keys[25], (D,), jnp.float32) ** steps_of(arg_keys[25], (D,), ((0, 4),), -0.2, 0.2), 0.3, 1.5)
    return {"tokens": tokens, "mixer_gain": mixer_gain, "gate_weight": gate_weight, "inner_weight": inner_weight, "state_weight": state_weight, "step_weight": step_weight, "step_bias": step_bias, "decay_log": decay_log, "skip_scale": skip_scale, "inner_kernel": inner_kernel, "state_kernel": state_kernel, "inner_window": inner_window, "state_window": state_window, "recurrent_state": recurrent_state, "group_gain": group_gain, "output_weight": output_weight, "channel_gain": channel_gain, "routes": routes, "route_weights": route_weights, "expert_gate": expert_gate, "expert_up": expert_up, "expert_down": expert_down, "dense_gate": dense_gate, "dense_up": dense_up, "dense_down": dense_down, "dense_scale": dense_scale}


eps = 1e-06

def rms_scale(values, norm_gain):
    squares = lax.optimization_barrier(jnp.mean(values * values, axis=-1, keepdims=True))
    return values * lax.rsqrt(squares + eps) * norm_gain

def reference(tokens, mixer_gain, gate_weight, inner_weight, state_weight, step_weight, step_bias, decay_log, skip_scale, inner_kernel, state_kernel, inner_window, state_window, recurrent_state, group_gain, output_weight, channel_gain, routes, route_weights, expert_gate, expert_up, expert_down, dense_gate, dense_up, dense_down, dense_scale):
    f32 = jnp.float32
    bf16 = jnp.bfloat16
    residual = tokens.astype(f32)
    normed = rms_scale(residual, mixer_gain).astype(bf16)
    gate_pre = jnp.dot(normed, gate_weight, preferred_element_type=f32)
    inner_pre = jnp.dot(normed, inner_weight, preferred_element_type=f32).astype(bf16)
    state_pre = jnp.stack([jnp.dot(normed, state_weight[0], preferred_element_type=f32), jnp.dot(normed, state_weight[1], preferred_element_type=f32)], axis=1).astype(bf16)
    step_raw = jnp.dot(normed, step_weight, preferred_element_type=f32)
    inner_ctx = jnp.concatenate([inner_window, inner_pre[:, None, :]], axis=1)
    inner_conv = jax.nn.silu(lax.optimization_barrier(jnp.sum(inner_ctx.astype(f32) * inner_kernel[None], axis=1)))
    state_ctx = jnp.concatenate([state_window, state_pre[:, None]], axis=1)
    state_conv = jax.nn.silu(lax.optimization_barrier(jnp.sum(state_ctx.astype(f32) * state_kernel[None], axis=1)))
    per_group = HEADS // GROUPS
    step_size = jax.nn.softplus(step_raw + step_bias)
    decay_rate = jnp.exp(-step_size * jnp.exp(decay_log))
    shaped = (BATCH, GROUPS, per_group)
    inner_heads = inner_conv.reshape(BATCH, GROUPS, per_group, HEAD_DIM)
    in_vector = state_conv[:, 0].reshape(BATCH, GROUPS, STATE_DIM)
    out_vector = state_conv[:, 1].reshape(BATCH, GROUPS, STATE_DIM)
    old_state = recurrent_state.reshape(BATCH, GROUPS, per_group, HEAD_DIM, STATE_DIM)
    written = (step_size.reshape(shaped)[..., None] * inner_heads)[..., None] * in_vector[:, :, None, None, :]
    new_state = old_state * decay_rate.reshape(shaped)[..., None, None] + written
    mixed_out = jnp.einsum('sgrpn,sgn->sgrp', new_state, out_vector, precision=lax.Precision.HIGHEST)
    mixed_out = mixed_out + skip_scale.reshape(GROUPS, per_group)[None, :, :, None] * inner_heads
    gated_out = mixed_out.reshape(BATCH, INNER) * jax.nn.silu(gate_pre)
    grouped = rms_scale(gated_out.reshape(BATCH, GROUPS, -1), 1.0).reshape(BATCH, INNER)
    mixer_rows = (grouped * group_gain).astype(bf16)
    block_width = INNER // N_TP
    mixer_out = jnp.zeros((BATCH, D), f32)
    for block_index in range(N_TP):
        part_sum = jnp.dot(mixer_rows[:, block_index * block_width:(block_index + 1) * block_width], output_weight[block_index * block_width:(block_index + 1) * block_width], preferred_element_type=f32)
        mixer_out = mixer_out + lax.optimization_barrier(part_sum.astype(bf16)).astype(f32)
    residual = residual + mixer_out
    ffn_rows = rms_scale(residual, channel_gain).astype(bf16)
    dense_hidden = (jax.nn.silu(jnp.dot(ffn_rows, dense_gate, preferred_element_type=f32)) * jnp.dot(ffn_rows, dense_up, preferred_element_type=f32)).astype(bf16)
    dense_out = jnp.dot(dense_hidden, dense_down, preferred_element_type=f32)
    entries = S_DEV * TOPK
    flat_routes = routes.reshape(N_EP, entries)
    onehot = (flat_routes[:, :, None] == jnp.arange(EXPERTS, dtype=jnp.int32)[None, None, :]).astype(jnp.int32)
    rank_before = jnp.cumsum(onehot, axis=1) - onehot
    slot_index = lax.optimization_barrier(jnp.sum(rank_before * onehot, axis=2)).astype(jnp.int32)
    block_rows = ffn_rows.astype(f32).reshape(N_EP, S_DEV, D)
    hidden_width = FF // N_TP

    def one_expert(expert_id):
        chosen = (flat_routes == expert_id)[:, None, :] & (slot_index[:, None, :] == jnp.arange(CAP, dtype=jnp.int32)[None, :, None])
        chosen = lax.optimization_barrier(jnp.sum(chosen.astype(f32).reshape(N_EP, CAP, S_DEV, TOPK), axis=3))
        gathered = jnp.einsum('bcs,bsd->bcd', chosen, block_rows).astype(bf16).reshape(N_EP * CAP, D)
        gate_act = jnp.dot(gathered, expert_gate[expert_id], preferred_element_type=f32)
        up_act = jnp.dot(gathered, expert_up[expert_id], preferred_element_type=f32)
        activated = (jax.nn.silu(gate_act) * up_act).astype(bf16)
        down_whole = expert_down[expert_id]
        total = jnp.zeros((N_EP * CAP, D), f32)
        for block_index in range(N_TP):
            part_sum = jnp.dot(activated[:, block_index * hidden_width:(block_index + 1) * hidden_width], down_whole[block_index * hidden_width:(block_index + 1) * hidden_width], preferred_element_type=f32)
            total = total + lax.optimization_barrier(part_sum.astype(bf16)).astype(f32)
        return total.astype(bf16).reshape(N_EP, CAP, D)
    expert_rows = lax.map(one_expert, jnp.arange(EXPERTS, dtype=jnp.int32))
    block_ids = jnp.broadcast_to(jnp.arange(N_EP, dtype=jnp.int32)[:, None], (N_EP, entries))
    picked = expert_rows[flat_routes, block_ids, slot_index].astype(f32)
    weighted = picked.reshape(N_EP, S_DEV, TOPK, D) * route_weights.reshape(N_EP, S_DEV, TOPK)[..., None]
    expert_out = lax.optimization_barrier(jnp.sum(weighted, axis=2)).reshape(BATCH, D)
    new_tokens = (residual + expert_out + dense_scale * dense_out).astype(bf16)
    return (new_tokens, new_state.reshape(BATCH, HEADS, HEAD_DIM, STATE_DIM), inner_ctx[:, 1:], state_ctx[:, 1:])
```

```python
import functools

import jax
import jax.numpy as jnp
from jax import lax
from jax.experimental import pallas as pl
from jax.experimental.pallas import tpu as pltpu
from jax.sharding import PartitionSpec as P

HEADS = 16
GROUPS = 4
HEAD_DIM = 64
STATE_DIM = 128
LANES = 128
SEQ_STEP = 4

eps = 1e-06


def silu(v):
    return v / (1.0 + jnp.exp(-v))


def dot_rows(rows, columns):
    return lax.dot_general(
        rows, columns, (((1,), (1,)), ((), ())), preferred_element_type=jnp.float32
    )


def dot(a, b):
    return jnp.dot(a, b, preferred_element_type=jnp.float32)


def mixer(
    tokens_hbm,
    mgain_hbm,
    gatew_hbm,
    innerw_hbm,
    statew_hbm,
    stepw_hbm,
    sbias_hbm,
    dlog_hbm,
    skip_hbm,
    ikern_hbm,
    skern_hbm,
    iwin_hbm,
    swin_hbm,
    state_hbm,
    ggain_hbm,
    rows_out,
    state_out,
    iwin_out,
    swin_out,
    tokens,
    mgain,
    gatew,
    innerw,
    statew,
    stepw,
    sbias,
    dlog,
    skip,
    ikern,
    skern,
    iwin,
    swin,
    state,
    ggain,
    decays,
    mixed,
    rows,
    sems,
    state_sems,
    out_sems,
):
    f32 = jnp.float32
    bf16 = jnp.bfloat16
    count = tokens.shape[0]
    taps = ikern.shape[0]
    heads = sbias.shape[1]
    inner = innerw.shape[1]
    head_dim = inner // heads
    n_state = statew.shape[2]
    small = [
        (tokens_hbm, tokens),
        (mgain_hbm, mgain),
        (innerw_hbm, innerw),
        (statew_hbm, statew),
        (stepw_hbm, stepw),
        (sbias_hbm, sbias),
        (dlog_hbm, dlog),
        (ikern_hbm, ikern),
        (skern_hbm, skern),
        (iwin_hbm, iwin.at[pl.ds(0, taps - 1)]),
        (swin_hbm, swin.at[:, pl.ds(0, taps - 1)]),
        (gatew_hbm, gatew),
        (skip_hbm, skip),
        (ggain_hbm, ggain),
    ]
    loads = []
    for i, (src, dst) in enumerate(small):
        copy = pltpu.make_async_copy(src, dst, sems.at[i])
        copy.start()
        loads.append(copy)

    def state_load(i):
        at = pl.ds(i * SEQ_STEP, SEQ_STEP)
        return pltpu.make_async_copy(state_hbm.at[at], state.at[at], state_sems.at[0, i])

    def state_store(i):
        at = pl.ds(i * SEQ_STEP, SEQ_STEP)
        return pltpu.make_async_copy(state.at[at], state_out.at[at], state_sems.at[1, i])

    steps = count // SEQ_STEP
    for i in range(steps):
        state_load(i).start()

    loads[0].wait()
    loads[1].wait()
    value = tokens[...].astype(f32)
    squares = jnp.mean(value * value, axis=-1, keepdims=True)
    normed = (value * lax.rsqrt(squares + eps) * mgain[...]).astype(bf16)
    for i in range(2, 11):
        loads[i].wait()
    inner_pre = dot(normed, innerw[...]).astype(bf16)
    pre_u = dot(normed, statew[0])
    pre_c = dot(normed, statew[1])
    step_raw = dot_rows(normed, stepw[...])

    iwin[taps - 1] = inner_pre
    conv = inner_pre.astype(f32) * ikern[taps - 1 : taps, :]
    for j in range(taps - 1):
        conv = conv + iwin[j].astype(f32) * ikern[j : j + 1, :]
    inner_conv = silu(conv)

    both = jnp.concatenate([pre_u[:, None, :], pre_c[:, None, :]], axis=1).astype(bf16)
    swin[:, taps - 1] = both
    sconv = both.astype(f32) * skern[taps - 1][None]
    for j in range(taps - 1):
        sconv = sconv + swin[:, j].astype(f32) * skern[j][None]
    sconv = silu(sconv)
    u_vec = sconv[:, 0, :]
    c_vec = sconv[:, 1, :].astype(bf16)
    win_copies = [
        pltpu.make_async_copy(iwin.at[pl.ds(1, taps - 1)], iwin_out, out_sems.at[0]),
        pltpu.make_async_copy(swin.at[:, pl.ds(1, taps - 1)], swin_out, out_sems.at[1]),
    ]
    for copy in win_copies:
        copy.start()

    step_size = jax.nn.softplus(step_raw + sbias[...])
    decay = jnp.exp(-step_size * jnp.exp(dlog[...]))
    step_wide = jnp.concatenate(
        [jnp.broadcast_to(step_size[:, h : h + 1], (count, head_dim)) for h in range(heads)],
        axis=1,
    )
    for h in range(heads):
        decays[:, h * n_state : (h + 1) * n_state] = jnp.broadcast_to(
            decay[:, h : h + 1], (count, n_state)
        )
    written = (step_wide * inner_conv).T.astype(bf16)
    row_of = lax.broadcasted_iota(jnp.int32, (count, n_state), 0)
    mixed_row = lax.broadcasted_iota(jnp.int32, (count, inner), 0)
    mixed[...] = jnp.zeros_like(mixed)

    def update(i, carry):
        state_load(i).wait()
        total = mixed[...]
        for k in range(0, SEQ_STEP, 2):
            b = i * SEQ_STEP + k
            pair = jnp.concatenate(
                [jnp.where(row_of == b + n, u_vec, 0.0) for n in range(2)], axis=1
            ).astype(bf16)
            outer = dot(written, pair)
            for n in range(2):
                fade = decays[pl.ds(b + n, 1), :]
                parts = []
                for h in range(heads):
                    new = state[b + n, h] * fade[:, h * n_state : (h + 1) * n_state]
                    new = new + outer[
                        h * head_dim : (h + 1) * head_dim, n * n_state : (n + 1) * n_state
                    ]
                    state[b + n, h] = new
                    parts.append(new.astype(bf16))
                read = dot_rows(c_vec, jnp.concatenate(parts, axis=0))
                total = jnp.where(mixed_row == b + n, read, total)
        mixed[...] = total
        state_store(i).start()
        return carry

    lax.fori_loop(0, steps, update, 0)
    for i in range(11, 14):
        loads[i].wait()
    gate_pre = dot(normed, gatew[...])
    skip_wide = jnp.concatenate(
        [jnp.broadcast_to(skip[:, h : h + 1], (1, head_dim)) for h in range(heads)], axis=1
    )
    gated = (mixed[...] + skip_wide * inner_conv) * silu(gate_pre)
    squares = jnp.mean(gated * gated, axis=-1, keepdims=True)
    rows[...] = (gated * lax.rsqrt(squares + eps) * ggain[...]).astype(bf16)
    last = pltpu.make_async_copy(rows, rows_out, out_sems.at[2])
    last.start()
    for i in range(steps):
        state_store(i).wait()
    for copy in win_copies:
        copy.wait()
    last.wait()


def flip(index, mask):
    moved = index
    bit = 1
    while bit <= mask:
        if mask & bit:
            moved = moved + bit * (1 - 2 * lax.rem(index // bit, 2))
        bit *= 2
    return moved


def branches(
    ep_size,
    tp_size,
    slice_rows,
    rows_hbm,
    outw_hbm,
    tokens_hbm,
    gain_hbm,
    routes_hbm,
    rweights_hbm,
    scale_hbm,
    gate_hbm,
    up_hbm,
    down_hbm,
    dgate_hbm,
    dup_hbm,
    ddown_hbm,
    out,
    mrows,
    outw,
    tokens,
    gain,
    routes,
    rweights,
    scales,
    gate_w,
    up_w,
    down_w,
    dense_w,
    tables,
    part,
    parts,
    residual,
    rows,
    flat,
    packed,
    act,
    hid,
    y_part,
    y_recv,
    z_send,
    z_recv,
    load_sems,
    part_sems,
    table_sems,
    scale_sems,
    dense_sems,
    row_sems,
    relay_sems,
    y_sems,
    z_sems,
):
    f32 = jnp.float32
    bf16 = jnp.bfloat16
    me_e = lax.axis_index("ep")
    me_t = lax.axis_index("tp")
    side = me_t // 2
    core = lax.rem(me_t, 2)
    count, width = tokens.shape
    own_width = width // tp_size
    total = ep_size * count
    hidden_width = dgate_hbm.shape[0]
    halves = tp_size // 2

    def remote(src, dst, send, recv, to_e, to_t):
        return pltpu.make_async_remote_copy(
            src_ref=src,
            dst_ref=dst,
            send_sem=send,
            recv_sem=recv,
            device_id=(to_e, to_t),
            device_id_type=pl.DeviceIdType.MESH,
        )

    barrier = pltpu.get_barrier_semaphore()
    for m in range(1, tp_size):
        pl.semaphore_signal(
            barrier,
            inc=1,
            device_id=(me_e, flip(me_t, m)),
            device_id_type=pl.DeviceIdType.MESH,
        )
    for m in range(ep_size - 1, 0, -1):
        pl.semaphore_signal(
            barrier,
            inc=1,
            device_id=(flip(me_e, m), me_t),
            device_id_type=pl.DeviceIdType.MESH,
        )

    def dense_rows(ref, t):
        if slice_rows == hidden_width:
            return ref
        return ref.at[pl.ds(t * slice_rows, slice_rows)]

    dense_hbm = [dgate_hbm, dup_hbm, ddown_hbm]
    loads = []
    for src, dst in [
        (rows_hbm, mrows),
        (outw_hbm, outw),
        (tokens_hbm, tokens),
        (gain_hbm, gain),
        (routes_hbm, routes),
        (rweights_hbm, rweights),
        (scale_hbm, scales.at[me_t]),
        (gate_hbm, gate_w),
        (up_hbm, up_w),
        (down_hbm, down_w),
        (dense_rows(dgate_hbm, me_t), dense_w.at[0, me_t]),
        (dense_rows(dup_hbm, me_t), dense_w.at[1, me_t]),
        (dense_rows(ddown_hbm, me_t), dense_w.at[2, me_t]),
    ]:
        copy = pltpu.make_async_copy(src, dst, load_sems.at[len(loads)])
        copy.start()
        loads.append(copy)

    loads[0].wait()
    loads[1].wait()
    mixer_rows = mrows[...]
    for q in range(tp_size):
        piece = dot(mixer_rows, outw[:, q * own_width : (q + 1) * own_width])
        part[q % 2, q // 2] = piece.astype(bf16)
    loads[4].wait()
    loads[5].wait()
    expert_of = lax.broadcasted_iota(jnp.int32, (ep_size, count), 0)
    table = jnp.zeros((ep_size, count), f32)
    for k in range(routes.shape[0]):
        table = table + jnp.where(expert_of == routes[k : k + 1, :], rweights[k : k + 1, :], 0.0)
    tables[me_e] = jnp.concatenate([table, jnp.zeros((ep_size, LANES - count), f32)], axis=1)
    loads[2].wait()
    loads[6].wait()

    pl.semaphore_wait(barrier, ep_size + tp_size - 2)
    tp_order = [m for m in range(2, tp_size)] + [1]
    part_copies = {}
    for m in tp_order:
        to = flip(me_t, m)
        part_copies[m] = remote(
            part.at[lax.rem(to, 2)],
            parts.at[m],
            part_sems.at[0, m],
            part_sems.at[1, m],
            me_e,
            to,
        )
        part_copies[m].start()
    table_copies = []
    for m in range(1, ep_size):
        copy = remote(
            tables.at[me_e],
            tables.at[me_e],
            table_sems.at[0, m],
            table_sems.at[1, m],
            flip(me_e, m),
            me_t,
        )
        copy.start()
        table_copies.append(copy)
    dense_copies = []
    for m in tp_order:
        to = flip(me_t, m)
        copy = remote(
            scales.at[me_t],
            scales.at[me_t],
            scale_sems.at[0, m],
            scale_sems.at[1, m],
            me_e,
            to,
        )
        copy.start()
        dense_copies.append(copy)
        for k in range(3):
            copy = remote(
                dense_rows(dense_hbm[k], to),
                dense_w.at[k, me_t],
                dense_sems.at[0, k, m],
                dense_sems.at[1, k, m],
                me_e,
                to,
            )
            copy.start()
            dense_copies.append(copy)

    own_rows = []
    for h in range(halves):
        at = pl.ds(pl.multiple_of(core * own_width + 2 * h * own_width, own_width), own_width)
        own_rows.append(tokens[:, at].astype(f32) + part[core, h].astype(f32))
    for m in [1] + tp_order[:-1]:
        part_copies[m].wait_recv()
        for h in range(halves):
            own_rows[h] = own_rows[h] + parts[m, h].astype(f32)
    for h in range(halves):
        residual[h] = own_rows[h]
        rows[core, me_e, h] = own_rows[h].astype(bf16)

    row_copies = {}
    for m in range(ep_size - 1, 0, -1):
        row_copies[m] = remote(
            rows.at[core, me_e],
            rows.at[core, me_e],
            row_sems.at[0, m],
            row_sems.at[1, m],
            flip(me_e, m),
            me_t,
        )
        row_copies[m].start()
    partner = flip(me_t, 1)
    relay_copies = {}
    for m in range(ep_size):
        origin = flip(me_e, m)
        if m:
            row_copies[m].wait_recv()
        relay_copies[m] = remote(
            rows.at[core, origin],
            rows.at[core, origin],
            relay_sems.at[0, m],
            relay_sems.at[1, m],
            me_e,
            partner,
        )
        relay_copies[m].start()
    loads[3].wait()
    for m in range(ep_size):
        origin = flip(me_e, m)
        relay_copies[m].wait_recv()
        pieces = [rows[q % 2, origin, q // 2].astype(f32) for q in range(tp_size)]
        squares = pieces[0] * pieces[0]
        for q in range(1, tp_size):
            squares = squares + pieces[q] * pieces[q]
        scale_of = lax.rsqrt(jnp.sum(squares, axis=-1, keepdims=True) * (1.0 / width) + eps)
        at = pl.ds(pl.multiple_of(origin * count, count), count)
        for q in range(tp_size):
            lanes = slice(q * own_width, (q + 1) * own_width)
            flat[at, lanes] = pieces[q] * scale_of * gain[:, lanes]
    packed[...] = flat[...].astype(bf16)

    for i in range(7, 13):
        loads[i].wait()
    for copy in table_copies + dense_copies:
        copy.wait_recv()

    groups = 8 if ep_size % 8 == 0 else ep_size
    chunk = groups * count
    expert_hidden = gate_w.shape[1]
    unit = 64 if expert_hidden % 64 == 0 else expert_hidden
    if slice_rows == hidden_width:
        units = lax.broadcasted_iota(jnp.int32, (slice_rows, 1), 0)
        share = hidden_width // tp_size
        kept = (units // share == me_t).astype(f32)

    def activate(step, carry):
        at = pl.ds(pl.multiple_of(step * chunk, chunk), chunk)
        x = packed[at, :]
        for n in range(0, expert_hidden, unit):
            gate_act = dot_rows(gate_w[0, n : n + unit, :], x)
            up_act = dot_rows(up_w[0, n : n + unit, :], x)
            act[step, n : n + unit, :] = (silu(gate_act) * up_act).astype(bf16)
        gate_act = jnp.zeros((slice_rows, chunk), f32)
        up_act = jnp.zeros((slice_rows, chunk), f32)
        for t in range(tp_size):
            x_part = packed[at, t * own_width : (t + 1) * own_width]
            gate_act = gate_act + dot_rows(dense_w[0, t], x_part)
            up_act = up_act + dot_rows(dense_w[1, t], x_part)
        hidden = silu(gate_act) * up_act
        if slice_rows == hidden_width:
            hidden = hidden * kept
        hid[step] = hidden.astype(bf16)
        return carry

    lax.fori_loop(0, total // chunk, activate, 0)

    def weigh(b):
        held = tables[b]
        mine = lax.broadcasted_iota(jnp.int32, held.shape, 0) == me_e
        row = jnp.sum(jnp.where(mine, held, 0.0), axis=0, keepdims=True)[:, :count]
        diagonal = lax.broadcasted_iota(jnp.int32, (count, count), 0) == lax.broadcasted_iota(
            jnp.int32, (count, count), 1
        )
        return jnp.sum(jnp.where(diagonal, row, 0.0), axis=1, keepdims=True)

    contract_rows = (((0,), (0,)), ((), ()))

    def project(step, carry):
        acts = act[step]
        hidden = hid[step]
        weights = [weigh(step * groups + g) for g in range(groups)]
        for q in range(tp_size):
            lanes = slice(q * own_width, (q + 1) * own_width)
            routed = lax.dot_general(
                acts, down_w[0, :, lanes], contract_rows, preferred_element_type=f32
            )
            dense = lax.dot_general(
                hidden, dense_w[2, q], contract_rows, preferred_element_type=f32
            )
            for g in range(groups):
                at = slice(g * count, (g + 1) * count)
                y = routed[at] * weights[g] + dense[at] * scales[q]
                y_part[q % 2, q // 2, step * groups + g] = y.astype(bf16)
        return carry

    lax.fori_loop(0, total // chunk, project, 0)

    y_copies = []
    half_blocks = ep_size // 2
    top = me_e // half_blocks
    for k in range(2):
        which = (1 - top) if k == 0 else top
        at = pl.ds(which * half_blocks, half_blocks)
        copy = remote(
            y_part.at[1 - core, :, at],
            y_recv.at[:, at],
            y_sems.at[0, k],
            y_sems.at[1, k],
            me_e,
            partner,
        )
        copy.start()
        y_copies.append(copy)
    z_copies = []
    for k in range(2):
        y_copies[k].wait_recv()
        for m in range(ep_size // 2 * (2 - k) - 1, ep_size // 2 * (1 - k) - 1, -1):
            to = flip(me_e, m)
            for o in range(halves - 1, -1, -1):
                to_side = flip(side, o)
                summed = y_part[core, to_side, to].astype(f32) + y_recv[to_side, to].astype(f32)
                if m == 0 and o == 0:
                    final = residual[side] + summed
                    continue
                z_send[to_side, to] = summed.astype(bf16)
                copy = remote(
                    z_send.at[to_side, to],
                    z_recv.at[side, me_e],
                    z_sems.at[0, o, m],
                    z_sems.at[1, o, m],
                    to,
                    2 * to_side + core,
                )
                copy.start()
                z_copies.append((m, o, copy))
    for m, o, copy in sorted(z_copies, key=lambda item: item[:2]):
        copy.wait_recv()
        final = final + z_recv[flip(side, o), flip(me_e, m)].astype(f32)
    out[...] = final.astype(bf16)
    for copies in [part_copies, row_copies, relay_copies]:
        for copy in copies.values():
            copy.wait_send()
    for copy in table_copies + dense_copies + y_copies:
        copy.wait_send()
    for m, o, copy in z_copies:
        copy.wait_send()


def local(
    tokens,
    mixer_gain,
    gate_weight,
    inner_weight,
    state_weight,
    step_weight,
    step_bias,
    decay_log,
    skip_scale,
    inner_kernel,
    state_kernel,
    inner_window,
    state_window,
    recurrent_state,
    group_gain,
    output_weight,
    channel_gain,
    routes,
    route_weights,
    expert_gate,
    expert_up,
    expert_down,
    dense_gate,
    dense_up,
    dense_down,
    dense_scale,
):
    f32 = jnp.float32
    bf16 = jnp.bfloat16
    ep_size = lax.axis_size("ep")
    tp_size = lax.axis_size("tp")
    count, width = tokens.shape
    own_width = width // tp_size
    total = ep_size * count
    hbm = pl.BlockSpec(memory_space=pl.ANY)
    dma = pltpu.SemaphoreType.DMA
    vmem = pltpu.VMEM
    steps = count // SEQ_STEP

    inner_window = jnp.swapaxes(inner_window, 0, 1)
    taps = inner_kernel.shape[0]
    inner = inner_weight.shape[1]
    mixer_args = [
        tokens,
        mixer_gain[None],
        gate_weight,
        inner_weight,
        state_weight,
        step_weight.T,
        step_bias[None],
        decay_log[None],
        skip_scale[None],
        inner_kernel,
        state_kernel,
        inner_window,
        state_window,
        recurrent_state,
        group_gain[None],
    ]
    held = [vmem(a.shape, a.dtype) for a in mixer_args]
    held[11] = vmem((taps,) + inner_window.shape[1:], bf16)
    held[12] = vmem((count, taps) + state_window.shape[2:], bf16)
    heads = step_bias.shape[0]
    n_state = state_weight.shape[2]
    mixer_rows, new_state, new_inner, new_state_window = pl.pallas_call(
        mixer,
        out_shape=[
            jax.ShapeDtypeStruct((count, inner), bf16),
            jax.ShapeDtypeStruct(recurrent_state.shape, f32),
            jax.ShapeDtypeStruct(inner_window.shape, bf16),
            jax.ShapeDtypeStruct(state_window.shape, bf16),
        ],
        in_specs=[hbm] * len(mixer_args),
        out_specs=[hbm] * 4,
        scratch_shapes=held
        + [
            vmem((count, heads * n_state), f32),
            vmem((count, inner), f32),
            vmem((count, inner), bf16),
            dma((14,)),
            dma((2, steps)),
            dma((3,)),
        ],
        compiler_params=pltpu.CompilerParams(vmem_limit_bytes=60 * 1024 * 1024),
    )(*mixer_args)

    expert_gate = jnp.swapaxes(expert_gate, 1, 2)
    expert_up = jnp.swapaxes(expert_up, 1, 2)
    hidden_width = dense_gate.shape[1]
    slice_rows = hidden_width // tp_size
    if hidden_width % (8 * tp_size):
        slice_rows = hidden_width
    halves = tp_size // 2
    groups = 8 if ep_size % 8 == 0 else ep_size
    chunk = groups * count
    branch_args = [
        mixer_rows,
        output_weight,
        tokens,
        channel_gain[None],
        routes.T,
        route_weights.T,
        dense_scale[None],
        expert_gate,
        expert_up,
        expert_down,
        dense_gate.T,
        dense_up.T,
        dense_down,
    ]
    new_tokens = pl.pallas_call(
        functools.partial(branches, ep_size, tp_size, slice_rows),
        out_shape=jax.ShapeDtypeStruct((count, own_width), bf16),
        in_specs=[hbm] * len(branch_args),
        out_specs=pl.BlockSpec(memory_space=pltpu.VMEM),
        scratch_shapes=[vmem(a.shape, a.dtype) for a in branch_args[:6]]
        + [
            vmem((tp_size, 1, own_width), f32),
            vmem(expert_gate.shape, bf16),
            vmem(expert_up.shape, bf16),
            vmem(expert_down.shape, bf16),
            vmem((3, tp_size, slice_rows, own_width), bf16),
            vmem((ep_size, ep_size, LANES), f32),
            vmem((2, halves, count, own_width), bf16),
            vmem((tp_size, halves, count, own_width), bf16),
            vmem((halves, count, own_width), f32),
            vmem((2, ep_size, halves, count, own_width), bf16),
            vmem((total, width), f32),
            vmem((total, width), bf16),
            vmem((total // chunk, expert_gate.shape[1], chunk), bf16),
            vmem((total // chunk, slice_rows, chunk), bf16),
            vmem((2, halves, ep_size, count, own_width), bf16),
            vmem((halves, ep_size, count, own_width), bf16),
            vmem((halves, ep_size, count, own_width), bf16),
            vmem((halves, ep_size, count, own_width), bf16),
            dma((13,)),
            dma((2, tp_size)),
            dma((2, ep_size)),
            dma((2, tp_size)),
            dma((2, 3, tp_size)),
            dma((2, ep_size)),
            dma((2, ep_size)),
            dma((2, 2)),
            dma((2, halves, ep_size)),
        ],
        compiler_params=pltpu.CompilerParams(
            collective_id=0, has_side_effects=True, vmem_limit_bytes=60 * 1024 * 1024
        ),
    )(*branch_args)
    return (
        new_tokens,
        new_state,
        jnp.swapaxes(new_inner, 0, 1),
        new_state_window,
    )


def solution(mesh):
    placed = (
        P("ep", None),
        P(),
        P(None, "tp"),
        P(None, "tp"),
        P(None, None, "tp"),
        P(None, "tp"),
        P("tp"),
        P("tp"),
        P("tp"),
        P(None, "tp"),
        P(None, None, "tp"),
        P("ep", None, "tp"),
        P("ep", None, None, "tp"),
        P("ep", "tp", None, None),
        P("tp"),
        P("tp", None),
        P(),
        P("ep", None),
        P("ep", None),
        P("ep", None, "tp"),
        P("ep", None, "tp"),
        P("ep", "tp", None),
        P("tp", "ep"),
        P("tp", "ep"),
        P("ep", "tp"),
        P("tp"),
    )
    return jax.shard_map(
        local,
        mesh=mesh,
        in_specs=placed,
        out_specs=(
            P("ep", "tp"),
            P("ep", "tp", None, None),
            P("ep", None, "tp"),
            P("ep", None, None, "tp"),
        ),
        check_vma=False,
    )
```

```python
import functools

import jax
import jax.numpy as jnp
from jax import lax
from jax.experimental import pallas as pl
from jax.experimental.pallas import tpu as pltpu
from jax.sharding import PartitionSpec as P

HEADS = 16
GROUPS = 4
HEAD_DIM = 64
STATE_DIM = 128
LANES = 128
SEQ_STEP = 4
ROW_ORDER = (7, 6, 5, 4, 3, 2, 1)

eps = 1e-06


def silu(v):
    return v / (1.0 + jnp.exp(-v))


def dot_rows(rows, columns):
    return lax.dot_general(
        rows, columns, (((1,), (1,)), ((), ())), preferred_element_type=jnp.float32
    )


def dot(a, b):
    return jnp.dot(a, b, preferred_element_type=jnp.float32)


def mixer(
    tokens_hbm,
    mgain_hbm,
    gatew_hbm,
    innerw_hbm,
    statew_hbm,
    stepw_hbm,
    sbias_hbm,
    dlog_hbm,
    skip_hbm,
    ikern_hbm,
    skern_hbm,
    iwin_hbm,
    swin_hbm,
    state_hbm,
    ggain_hbm,
    rows_out,
    state_out,
    iwin_out,
    swin_out,
    tokens,
    mgain,
    gatew,
    innerw,
    statew,
    stepw,
    sbias,
    dlog,
    skip,
    ikern,
    skern,
    iwin,
    swin,
    state,
    ggain,
    decays,
    mixed,
    sems,
    state_sems,
    out_sems,
):
    f32 = jnp.float32
    bf16 = jnp.bfloat16
    count = tokens.shape[0]
    taps = ikern.shape[0]
    heads = sbias.shape[1]
    inner = innerw.shape[1]
    head_dim = inner // heads
    n_state = statew.shape[2]
    small = [
        (tokens_hbm, tokens),
        (mgain_hbm, mgain),
        (innerw_hbm, innerw),
        (statew_hbm, statew),
        (stepw_hbm, stepw),
        (sbias_hbm, sbias),
        (dlog_hbm, dlog),
        (ikern_hbm, ikern),
        (skern_hbm, skern),
        (iwin_hbm, iwin.at[pl.ds(0, taps - 1)]),
        (swin_hbm, swin.at[:, pl.ds(0, taps - 1)]),
        (gatew_hbm, gatew),
        (skip_hbm, skip),
        (ggain_hbm, ggain),
    ]
    loads = []
    for i, (src, dst) in enumerate(small):
        copy = pltpu.make_async_copy(src, dst, sems.at[i])
        copy.start()
        loads.append(copy)

    def state_load(i):
        at = pl.ds(i * SEQ_STEP, SEQ_STEP)
        return pltpu.make_async_copy(state_hbm.at[at], state.at[at], state_sems.at[0, i])

    def state_store(i):
        at = pl.ds(i * SEQ_STEP, SEQ_STEP)
        return pltpu.make_async_copy(state.at[at], state_out.at[at], state_sems.at[1, i])

    steps = count // SEQ_STEP
    loads[0].wait()
    loads[1].wait()
    for i in range(steps):
        state_load(i).start()
    value = tokens[...].astype(f32)
    squares = jnp.mean(value * value, axis=-1, keepdims=True)
    normed = (value * lax.rsqrt(squares + eps) * mgain[...]).astype(bf16)
    for i in range(2, 14):
        loads[i].wait()
    inner_pre = dot(normed, innerw[...]).astype(bf16)
    pre_u = dot(normed, statew[0])
    pre_c = dot(normed, statew[1])
    step_raw = dot_rows(normed, stepw[...])
    gate_pre = dot(normed, gatew[...])

    iwin[taps - 1] = inner_pre
    conv = inner_pre.astype(f32) * ikern[taps - 1 : taps, :]
    for j in range(taps - 1):
        conv = conv + iwin[j].astype(f32) * ikern[j : j + 1, :]
    inner_conv = silu(conv)

    both = jnp.concatenate([pre_u[:, None, :], pre_c[:, None, :]], axis=1).astype(bf16)
    swin[:, taps - 1] = both
    sconv = both.astype(f32) * skern[taps - 1][None]
    for j in range(taps - 1):
        sconv = sconv + swin[:, j].astype(f32) * skern[j][None]
    sconv = silu(sconv)
    u_vec = sconv[:, 0, :]
    c_vec = sconv[:, 1, :]
    win_copies = [
        pltpu.make_async_copy(iwin.at[pl.ds(1, taps - 1)], iwin_out, out_sems.at[0]),
        pltpu.make_async_copy(swin.at[:, pl.ds(1, taps - 1)], swin_out, out_sems.at[1]),
    ]
    for copy in win_copies:
        copy.start()

    step_size = jax.nn.softplus(step_raw + sbias[...])
    decay = jnp.exp(-step_size * jnp.exp(dlog[...]))
    step_wide = jnp.concatenate(
        [jnp.broadcast_to(step_size[:, h : h + 1], (count, head_dim)) for h in range(heads)],
        axis=1,
    )
    decay_wide = jnp.concatenate(
        [jnp.broadcast_to(decay[:, h : h + 1], (count, head_dim)) for h in range(heads)], axis=1
    )
    for h in range(heads):
        decays[:, h * n_state : (h + 1) * n_state] = jnp.broadcast_to(
            decay[:, h : h + 1], (count, n_state)
        )
    moved = step_wide * inner_conv
    written = moved.T.astype(bf16)
    row_of = lax.broadcasted_iota(jnp.int32, (count, n_state), 0)
    lane_of = lax.broadcasted_iota(jnp.int32, (inner, 2 * count), 1)
    none = jnp.zeros_like(c_vec)
    readers = jnp.concatenate(
        [jnp.concatenate([c_vec, none], axis=1), jnp.concatenate([none, c_vec], axis=1)], axis=0
    ).astype(bf16)

    for i in range(steps):
        state_load(i).wait()
        for b in range(i * SEQ_STEP, (i + 1) * SEQ_STEP, 2):
            pair = jnp.concatenate(
                [jnp.where(row_of == b + n, u_vec, 0.0) for n in range(2)], axis=1
            ).astype(bf16)
            outer = dot(written, pair)
            old = [
                jnp.concatenate([state[b + n, h].astype(bf16) for h in range(heads)], axis=0)
                for n in range(2)
            ]
            read = dot_rows(jnp.concatenate(old, axis=1), readers)
            if b:
                read = jnp.where((lane_of == b) | (lane_of == count + b + 1), read, mixed[...])
            mixed[...] = read
            for n in range(2):
                for h in range(heads):
                    fade = decays[b + n : b + n + 1, h * n_state : (h + 1) * n_state]
                    state[b + n, h] = (
                        state[b + n, h] * fade
                        + outer[h * head_dim : (h + 1) * head_dim, n * n_state : (n + 1) * n_state]
                    )
        state_store(i).start()

    read = mixed[...].T
    even = lax.rem(lax.broadcasted_iota(jnp.int32, (count, inner), 0), 2) == 0
    read = jnp.where(even, read[:count], read[count:])
    mixed_out = decay_wide * read + moved * jnp.sum(u_vec * c_vec, axis=1, keepdims=True)
    skip_wide = jnp.concatenate(
        [jnp.broadcast_to(skip[:, h : h + 1], (1, head_dim)) for h in range(heads)], axis=1
    )
    gated = (mixed_out + skip_wide * inner_conv) * silu(gate_pre)
    squares = jnp.mean(gated * gated, axis=-1, keepdims=True)
    rows_out[...] = (gated * lax.rsqrt(squares + eps) * ggain[...]).astype(bf16)
    for i in range(steps):
        state_store(i).wait()
    for copy in win_copies:
        copy.wait()


def padded(rows):
    return -(-rows // 16) * 16


def flipped(a, b):
    low = lax.rem(a + b, 2)
    high = lax.rem(a // 2 + b // 2, 2)
    return 2 * high + low


def flip(index, mask):
    moved = index
    bit = 1
    while bit <= mask:
        if mask & bit:
            moved = moved + bit * (1 - 2 * lax.rem(index // bit, 2))
        bit *= 2
    return moved


def branches(
    ep_size,
    tp_size,
    slice_rows,
    chunks,
    mrows,
    outw,
    tokens,
    gain,
    routes,
    rweights,
    scale,
    gate_hbm,
    up_hbm,
    down_hbm,
    dgate_hbm,
    dup_hbm,
    ddown_hbm,
    out,
    scales,
    weights_in,
    down_w,
    dense_w,
    tables,
    part,
    parts,
    residual,
    rows,
    flat,
    pre,
    act,
    y_part,
    y_recv,
    z_send,
    z_recv,
    load_sems,
    part_sems,
    table_sems,
    scale_sems,
    dense_sems,
    row_send,
    row_sems,
    relay_send,
    relay_sems,
    y_sems,
    z_sems,
):
    f32 = jnp.float32
    bf16 = jnp.bfloat16
    me_e = lax.axis_index("ep")
    me_t = lax.axis_index("tp")
    side = me_t // 2
    core = lax.rem(me_t, 2)
    partner = flip(me_t, 1)
    count, width = tokens.shape
    own_width = width // tp_size
    hidden_width = dgate_hbm.shape[0]
    halves = tp_size // 2
    expert_hidden = gate_hbm.shape[1]
    dense_at = [2 * expert_hidden, 2 * expert_hidden + padded(slice_rows)]

    def remote(src, dst, send, recv, to_e, to_t):
        copy = pltpu.make_async_remote_copy(
            src_ref=src,
            dst_ref=dst,
            send_sem=send,
            recv_sem=recv,
            device_id=(to_e, to_t),
            device_id_type=pl.DeviceIdType.MESH,
        )
        copy.start()
        return copy

    def settle(ref, sem):
        pltpu.make_async_copy(ref, ref, sem).wait()

    barrier = pltpu.get_barrier_semaphore()
    for m in range(1, tp_size):
        pl.semaphore_signal(
            barrier,
            inc=1,
            device_id=(me_e, flip(me_t, m)),
            device_id_type=pl.DeviceIdType.MESH,
        )
    for m in range(ep_size - 1, 0, -1):
        pl.semaphore_signal(
            barrier,
            inc=1,
            device_id=(flip(me_e, m), me_t),
            device_id_type=pl.DeviceIdType.MESH,
        )

    def dense_rows(ref, t):
        if slice_rows == hidden_width:
            return ref
        return ref.at[pl.ds(t * slice_rows, slice_rows)]

    dense_hbm = [dgate_hbm, dup_hbm, ddown_hbm]
    for src, dst, sem in [
        (gate_hbm.at[0], weights_in.at[pl.ds(0, expert_hidden)], 0),
        (up_hbm.at[0], weights_in.at[pl.ds(expert_hidden, expert_hidden)], 0),
        (down_hbm.at[0], down_w, 1),
    ] + [(dense_rows(dense_hbm[k], me_t), dense_w.at[0, k], 2) for k in range(3)]:
        pltpu.make_async_copy(src, dst, load_sems.at[sem]).start()

    mixer_rows = mrows[...]
    for q in range(tp_size):
        piece = dot(mixer_rows, outw[:, q * own_width : (q + 1) * own_width])
        part[q % 2, q // 2] = piece.astype(bf16)
    expert_of = lax.broadcasted_iota(jnp.int32, (ep_size, count), 0)
    table = jnp.zeros((ep_size, count), f32)
    for k in range(routes.shape[0]):
        table = table + jnp.where(expert_of == routes[k : k + 1, :], rweights[k : k + 1, :], 0.0)
    tables[0] = jnp.concatenate([table, jnp.zeros((ep_size, LANES - count), f32)], axis=1)
    scales[0] = scale[...]

    pl.semaphore_wait(barrier, ep_size + tp_size - 2)
    tp_order = [m for m in range(2, tp_size)] + [1]
    for m in tp_order:
        to = flip(me_t, m)
        remote(
            part.at[lax.rem(to, 2)], parts.at[m], part_sems.at[0], part_sems.at[1], me_e, to
        )
    for m in range(1, ep_size):
        remote(
            tables.at[0], tables.at[m], table_sems.at[0], table_sems.at[1], flip(me_e, m), me_t
        )
    for m in tp_order:
        to = flip(me_t, m)
        remote(scales.at[0], scales.at[m], scale_sems.at[0], scale_sems.at[1], me_e, to)
        for k in range(3):
            remote(
                dense_rows(dense_hbm[k], to),
                dense_w.at[m, k],
                dense_sems.at[0],
                dense_sems.at[1],
                me_e,
                to,
            )

    own_rows = []
    for h in range(halves):
        at = pl.ds(pl.multiple_of(core * own_width + 2 * h * own_width, own_width), own_width)
        own_rows.append(tokens[:, at].astype(f32) + part[core, h].astype(f32))
    settle(parts.at[pl.ds(1, tp_size - 1)], part_sems.at[1])
    for h in range(halves):
        for m in range(1, tp_size):
            own_rows[h] = own_rows[h] + parts[m, h].astype(f32)
        residual[h] = own_rows[h]
        rows[core, 0, h] = own_rows[h].astype(bf16)

    row_copies = {}
    for m in ROW_ORDER if ep_size == 8 else range(1, ep_size):
        row_copies[m] = remote(
            rows.at[core, 0],
            rows.at[core, m],
            row_send.at[0],
            row_sems.at[m],
            flip(me_e, m),
            me_t,
        )

    relay_copies = {}

    def relay(m):
        if m:
            row_copies[m].wait_recv()
        relay_copies[m] = remote(
            rows.at[core, m],
            rows.at[core, m],
            relay_send.at[0],
            relay_sems.at[m],
            me_e,
            partner,
        )

    def normalize(m, at):
        relay_copies[m].wait_recv()
        pieces = [rows[q % 2, m, q // 2].astype(f32) for q in range(tp_size)]
        squares = pieces[0] * pieces[0]
        for q in range(1, tp_size):
            squares = squares + pieces[q] * pieces[q]
        scale_of = lax.rsqrt(jnp.sum(squares, axis=-1, keepdims=True) * (1.0 / width) + eps)
        for q in range(tp_size):
            lanes = slice(q * own_width, (q + 1) * own_width)
            flat[at * count : (at + 1) * count, lanes] = pieces[q] * scale_of * gain[:, lanes]

    unit = 64 if expert_hidden % 64 == 0 else expert_hidden
    if slice_rows == hidden_width:
        units = lax.broadcasted_iota(jnp.int32, (slice_rows, 1), 0)
        share = hidden_width // tp_size
        kept = (units // share == me_t).astype(f32)

    def place_weights():
        settle(weights_in.at[pl.ds(0, 2 * expert_hidden)], load_sems.at[0])
        settle(down_w, load_sems.at[1])
        settle(dense_w.at[0], load_sems.at[2])
        settle(tables.at[pl.ds(1, ep_size - 1)], table_sems.at[1])
        settle(scales.at[pl.ds(1, tp_size - 1)], scale_sems.at[1])
        settle(dense_w.at[pl.ds(1, tp_size - 1)], dense_sems.at[1])
        for k in range(2):
            at = slice(dense_at[k], dense_at[k] + slice_rows)
            for m in range(tp_size):
                lanes = pl.ds(pl.multiple_of(flip(me_t, m) * own_width, own_width), own_width)
                weights_in[at, lanes] = dense_w[m, k]

    def activate(chunk):
        live = len(chunk) * count
        lanes = slice(0, live)
        x = flat[:live, :].astype(bf16)
        pre[:, lanes] = dot_rows(weights_in[...], x)
        for n in range(0, expert_hidden, unit):
            gate_act = pre[n : n + unit, lanes]
            up_act = pre[expert_hidden + n : expert_hidden + n + unit, lanes]
            act[n : n + unit, lanes] = (silu(gate_act) * up_act).astype(bf16)
        gate_act = pre[dense_at[0] : dense_at[0] + slice_rows, lanes]
        up_act = pre[dense_at[1] : dense_at[1] + slice_rows, lanes]
        hidden = silu(gate_act) * up_act
        if slice_rows == hidden_width:
            hidden = hidden * kept
        act[expert_hidden : expert_hidden + slice_rows, lanes] = hidden.astype(bf16)

    def weigh(m):
        held = tables[m]
        mine = lax.broadcasted_iota(jnp.int32, held.shape, 0) == me_e
        row = jnp.sum(jnp.where(mine, held, 0.0), axis=0, keepdims=True)[:, :count]
        diagonal = lax.broadcasted_iota(jnp.int32, (count, count), 0) == lax.broadcasted_iota(
            jnp.int32, (count, count), 1
        )
        return jnp.sum(jnp.where(diagonal, row, 0.0), axis=1, keepdims=True)

    contract_rows = (((0,), (0,)), ((), ()))

    def project(chunk, first):
        live = len(chunk) * count
        weights = [weigh(m) for m in chunk]
        acts = act[:expert_hidden, :live]
        hidden = act[expert_hidden : expert_hidden + slice_rows, :live]
        sent = None
        for mine in range(2):
            whose = core if mine else 1 - core
            for h in range(halves):
                t = 2 * h + whose
                lanes = pl.ds(pl.multiple_of(t * own_width, own_width), own_width)
                slot = flipped(me_t, t)
                routed = lax.dot_general(
                    acts, down_w[:, lanes], contract_rows, preferred_element_type=f32
                )
                dense = lax.dot_general(
                    hidden, dense_w[slot, 2], contract_rows, preferred_element_type=f32
                )
                for g in range(len(chunk)):
                    at = slice(g * count, (g + 1) * count)
                    y = routed[at] * weights[g] + dense[at] * scales[slot]
                    y_part[mine, h, first + g] = y.astype(bf16)
            if not mine:
                at = pl.ds(first, len(chunk))
                sent = remote(
                    y_part.at[0, :, at],
                    y_recv.at[:, at],
                    y_sems.at[0, len(y_copies)],
                    y_sems.at[1, len(y_copies)],
                    me_e,
                    partner,
                )
        y_copies.append(sent)

    def give_back(chunk, first, sent):
        sent.wait_recv()
        kept_sum = None
        for g in reversed(range(len(chunk))):
            m = chunk[g]
            for o in range(halves - 1, -1, -1):
                to_side = flip(side, o)
                summed = y_part[1, to_side, first + g].astype(f32)
                summed = summed + y_recv[to_side, first + g].astype(f32)
                if m == 0 and o == 0:
                    kept_sum = summed
                    continue
                z_send[o * ep_size + m] = summed.astype(bf16)
                remote(
                    z_send.at[o * ep_size + m],
                    z_recv.at[o * ep_size + m],
                    z_sems.at[0],
                    z_sems.at[1],
                    flip(me_e, m),
                    2 * to_side + core,
                )
        return kept_sum

    y_copies = []
    firsts = [sum(len(c) for c in chunks[:k]) for k in range(len(chunks))]
    for m in chunks[0]:
        relay(m)
    for at, m in enumerate(chunks[0]):
        normalize(m, at)
    place_weights()
    activate(chunks[0])
    final = None
    for k, chunk in enumerate(chunks):
        after = chunks[k + 1] if k + 1 < len(chunks) else []
        for m in after:
            relay(m)
        project(chunk, firsts[k])
        for at, m in enumerate(after):
            normalize(m, at)
        if after:
            activate(after)
        kept_sum = give_back(chunk, firsts[k], y_copies[k])
        if kept_sum is not None:
            final = residual[side] + kept_sum

    settle(z_recv.at[pl.ds(1, halves * ep_size - 1)], z_sems.at[1])
    for o in range(halves):
        for m in range(ep_size):
            if m or o:
                final = final + z_recv[o * ep_size + m].astype(f32)
    out[...] = final.astype(bf16)

    settle(parts.at[pl.ds(1, tp_size - 1)], part_sems.at[0])
    settle(tables.at[pl.ds(1, ep_size - 1)], table_sems.at[0])
    settle(scales.at[pl.ds(1, tp_size - 1)], scale_sems.at[0])
    settle(dense_w.at[pl.ds(1, tp_size - 1)], dense_sems.at[0])
    settle(rows.at[0, pl.ds(1, ep_size - 1)], row_send.at[0])
    settle(rows.at[0], relay_send.at[0])
    for copy in y_copies:
        copy.wait_send()
    settle(z_send.at[pl.ds(1, halves * ep_size - 1)], z_sems.at[0])


def local(
    tokens,
    mixer_gain,
    gate_weight,
    inner_weight,
    state_weight,
    step_weight,
    step_bias,
    decay_log,
    skip_scale,
    inner_kernel,
    state_kernel,
    inner_window,
    state_window,
    recurrent_state,
    group_gain,
    output_weight,
    channel_gain,
    routes,
    route_weights,
    expert_gate,
    expert_up,
    expert_down,
    dense_gate,
    dense_up,
    dense_down,
    dense_scale,
):
    f32 = jnp.float32
    bf16 = jnp.bfloat16
    ep_size = lax.axis_size("ep")
    tp_size = lax.axis_size("tp")
    count, width = tokens.shape
    own_width = width // tp_size
    hbm = pl.BlockSpec(memory_space=pltpu.HBM)
    on_chip = pl.BlockSpec(memory_space=pltpu.VMEM)
    dma = pltpu.SemaphoreType.DMA
    vmem = pltpu.VMEM
    steps = count // SEQ_STEP

    inner_window = jnp.swapaxes(inner_window, 0, 1)
    taps = inner_kernel.shape[0]
    inner = inner_weight.shape[1]
    mixer_args = [
        tokens,
        mixer_gain[None],
        gate_weight,
        inner_weight,
        state_weight,
        step_weight.T,
        step_bias[None],
        decay_log[None],
        skip_scale[None],
        inner_kernel,
        state_kernel,
        inner_window,
        state_window,
        recurrent_state,
        group_gain[None],
    ]
    held = [vmem(a.shape, a.dtype) for a in mixer_args]
    held[11] = vmem((taps,) + inner_window.shape[1:], bf16)
    held[12] = vmem((count, taps) + state_window.shape[2:], bf16)
    heads = step_bias.shape[0]
    n_state = state_weight.shape[2]
    mixer_rows, new_state, new_inner, new_state_window = pl.pallas_call(
        mixer,
        out_shape=[
            jax.ShapeDtypeStruct((count, inner), bf16),
            jax.ShapeDtypeStruct(recurrent_state.shape, f32),
            jax.ShapeDtypeStruct(inner_window.shape, bf16),
            jax.ShapeDtypeStruct(state_window.shape, bf16),
        ],
        in_specs=[hbm] * len(mixer_args),
        out_specs=[on_chip] + [hbm] * 3,
        scratch_shapes=held
        + [
            vmem((count, heads * n_state), f32),
            vmem((inner, 2 * count), f32),
            dma((14,)),
            dma((2, steps)),
            dma((2,)),
        ],
        compiler_params=pltpu.CompilerParams(vmem_limit_bytes=24 * 1024 * 1024),
    )(*[pltpu.with_memory_space_constraint(a, pltpu.HBM) for a in mixer_args])

    expert_gate = jnp.swapaxes(expert_gate, 1, 2)
    expert_up = jnp.swapaxes(expert_up, 1, 2)
    hidden_width = dense_gate.shape[1]
    expert_hidden = expert_gate.shape[1]
    slice_rows = hidden_width // tp_size
    if hidden_width % (8 * tp_size):
        slice_rows = hidden_width
    halves = tp_size // 2
    chunk_len = min(ep_size, 4 if ep_size <= 8 else 8)
    chunks = [list(range(k, k + chunk_len)) for k in range(0, ep_size, chunk_len)]
    live = chunk_len * count
    wide = 2 * (expert_hidden + padded(slice_rows))
    branch_args = [
        mixer_rows,
        output_weight,
        tokens,
        channel_gain[None],
        routes.T,
        route_weights.T,
        dense_scale[None],
        expert_gate,
        expert_up,
        expert_down,
        dense_gate.T,
        dense_up.T,
        dense_down,
    ]
    new_tokens = pl.pallas_call(
        functools.partial(branches, ep_size, tp_size, slice_rows, chunks),
        out_shape=jax.ShapeDtypeStruct((count, own_width), bf16),
        in_specs=[on_chip] * 7 + [hbm] * (len(branch_args) - 7),
        out_specs=pl.BlockSpec(memory_space=pltpu.VMEM),
        scratch_shapes=[
            vmem((tp_size, 1, own_width), f32),
            vmem((wide, width), bf16),
            vmem(expert_down.shape[1:], bf16),
            vmem((tp_size, 3, slice_rows, own_width), bf16),
            vmem((ep_size, ep_size, LANES), f32),
            vmem((2, halves, count, own_width), bf16),
            vmem((tp_size, halves, count, own_width), bf16),
            vmem((halves, count, own_width), f32),
            vmem((2, ep_size, halves, count, own_width), bf16),
            vmem((live, width), f32),
            vmem((wide, live), f32),
            vmem((expert_hidden + padded(slice_rows), live), bf16),
            vmem((2, halves, ep_size, count, own_width), bf16),
            vmem((halves, ep_size, count, own_width), bf16),
            vmem((halves * ep_size, count, own_width), bf16),
            vmem((halves * ep_size, count, own_width), bf16),
            dma((3,)),
            dma((2,)),
            dma((2,)),
            dma((2,)),
            dma((2,)),
            dma((1,)),
            dma((ep_size,)),
            dma((1,)),
            dma((ep_size,)),
            dma((2, len(chunks))),
            dma((2,)),
        ],
        compiler_params=pltpu.CompilerParams(
            collective_id=0, has_side_effects=True, vmem_limit_bytes=(24 if ep_size <= 8 else 56) * 1024 * 1024
        ),
    )(*branch_args[:7], *[pltpu.with_memory_space_constraint(a, pltpu.HBM) for a in branch_args[7:]])
    return (
        new_tokens,
        new_state,
        jnp.swapaxes(new_inner, 0, 1),
        new_state_window,
    )


def solution(mesh):
    placed = (
        P("ep", None),
        P(),
        P(None, "tp"),
        P(None, "tp"),
        P(None, None, "tp"),
        P(None, "tp"),
        P("tp"),
        P("tp"),
        P("tp"),
        P(None, "tp"),
        P(None, None, "tp"),
        P("ep", None, "tp"),
        P("ep", None, None, "tp"),
        P("ep", "tp", None, None),
        P("tp"),
        P("tp", None),
        P(),
        P("ep", None),
        P("ep", None),
        P("ep", None, "tp"),
        P("ep", None, "tp"),
        P("ep", "tp", None),
        P("tp", "ep"),
        P("tp", "ep"),
        P("ep", "tp"),
        P("tp"),
    )
    return jax.shard_map(
        local,
        mesh=mesh,
        in_specs=placed,
        out_specs=(
            P("ep", "tp"),
            P("ep", "tp", None, None),
            P("ep", None, "tp"),
            P("ep", None, None, "tp"),
        ),
        check_vma=False,
    )
```

```python
import functools

import jax
import jax.numpy as jnp
from jax import lax
from jax.experimental import pallas as pl
from jax.experimental.pallas import tpu as pltpu
from jax.sharding import PartitionSpec as P

HEADS = 16
GROUPS = 4
HEAD_DIM = 64
STATE_DIM = 128
LANES = 128
SEQ_STEP = 4
RELAY_LAG = 8
CHUNKS = ((0, 8),)

eps = 1e-06


def silu(v):
    return v / (1.0 + jnp.exp(-v))


def dot_rows(rows, columns):
    return lax.dot_general(
        rows, columns, (((1,), (1,)), ((), ())), preferred_element_type=jnp.float32
    )


def dot(a, b):
    return jnp.dot(a, b, preferred_element_type=jnp.float32)


def mixer(
    tokens_hbm,
    mgain_hbm,
    gatew_hbm,
    innerw_hbm,
    statew_hbm,
    stepw_hbm,
    sbias_hbm,
    dlog_hbm,
    skip_hbm,
    ikern_hbm,
    skern_hbm,
    iwin_hbm,
    swin_hbm,
    state_hbm,
    ggain_hbm,
    rows_out,
    state_out,
    iwin_out,
    swin_out,
    tokens,
    mgain,
    gatew,
    innerw,
    statew,
    stepw,
    sbias,
    dlog,
    skip,
    ikern,
    skern,
    iwin,
    swin,
    state,
    ggain,
    decays,
    mixed,
    sems,
    state_sems,
    out_sems,
):
    f32 = jnp.float32
    bf16 = jnp.bfloat16
    count = tokens.shape[0]
    taps = ikern.shape[0]
    heads = sbias.shape[1]
    inner = innerw.shape[1]
    head_dim = inner // heads
    n_state = statew.shape[2]
    small = [
        (tokens_hbm, tokens),
        (mgain_hbm, mgain),
        (innerw_hbm, innerw),
        (statew_hbm, statew),
        (stepw_hbm, stepw),
        (sbias_hbm, sbias),
        (dlog_hbm, dlog),
        (ikern_hbm, ikern),
        (skern_hbm, skern),
        (iwin_hbm, iwin.at[pl.ds(0, taps - 1)]),
        (swin_hbm, swin.at[:, pl.ds(0, taps - 1)]),
        (gatew_hbm, gatew),
        (skip_hbm, skip),
        (ggain_hbm, ggain),
    ]
    loads = []
    for i, (src, dst) in enumerate(small):
        copy = pltpu.make_async_copy(src, dst, sems.at[i])
        copy.start()
        loads.append(copy)

    def state_load(i):
        at = pl.ds(i * SEQ_STEP, SEQ_STEP)
        return pltpu.make_async_copy(state_hbm.at[at], state.at[at], state_sems.at[0, i])

    def state_store(i):
        at = pl.ds(i * SEQ_STEP, SEQ_STEP)
        return pltpu.make_async_copy(state.at[at], state_out.at[at], state_sems.at[1, i])

    steps = count // SEQ_STEP
    loads[0].wait()
    loads[1].wait()
    for i in range(steps):
        state_load(i).start()
    value = tokens[...].astype(f32)
    squares = jnp.mean(value * value, axis=-1, keepdims=True)
    normed = (value * lax.rsqrt(squares + eps) * mgain[...]).astype(bf16)
    for i in range(2, 14):
        loads[i].wait()
    inner_pre = dot(normed, innerw[...]).astype(bf16)
    pre_u = dot(normed, statew[0])
    pre_c = dot(normed, statew[1])
    step_raw = dot_rows(normed, stepw[...])
    gate_pre = dot(normed, gatew[...])

    iwin[taps - 1] = inner_pre
    conv = inner_pre.astype(f32) * ikern[taps - 1 : taps, :]
    for j in range(taps - 1):
        conv = conv + iwin[j].astype(f32) * ikern[j : j + 1, :]
    inner_conv = silu(conv)

    both = jnp.concatenate([pre_u[:, None, :], pre_c[:, None, :]], axis=1).astype(bf16)
    swin[:, taps - 1] = both
    sconv = both.astype(f32) * skern[taps - 1][None]
    for j in range(taps - 1):
        sconv = sconv + swin[:, j].astype(f32) * skern[j][None]
    sconv = silu(sconv)
    u_vec = sconv[:, 0, :]
    c_vec = sconv[:, 1, :]
    win_copies = [
        pltpu.make_async_copy(iwin.at[pl.ds(1, taps - 1)], iwin_out, out_sems.at[0]),
        pltpu.make_async_copy(swin.at[:, pl.ds(1, taps - 1)], swin_out, out_sems.at[1]),
    ]
    for copy in win_copies:
        copy.start()

    step_size = jax.nn.softplus(step_raw + sbias[...])
    decay = jnp.exp(-step_size * jnp.exp(dlog[...]))
    step_wide = jnp.concatenate(
        [jnp.broadcast_to(step_size[:, h : h + 1], (count, head_dim)) for h in range(heads)],
        axis=1,
    )
    decay_wide = jnp.concatenate(
        [jnp.broadcast_to(decay[:, h : h + 1], (count, head_dim)) for h in range(heads)], axis=1
    )
    for h in range(heads):
        decays[:, h * n_state : (h + 1) * n_state] = jnp.broadcast_to(
            decay[:, h : h + 1], (count, n_state)
        )
    moved = step_wide * inner_conv
    written = moved.T.astype(bf16)
    row_of = lax.broadcasted_iota(jnp.int32, (count, n_state), 0)
    lane_of = lax.broadcasted_iota(jnp.int32, (inner, 2 * count), 1)
    none = jnp.zeros_like(c_vec)
    readers = jnp.concatenate(
        [jnp.concatenate([c_vec, none], axis=1), jnp.concatenate([none, c_vec], axis=1)], axis=0
    ).astype(bf16)

    for i in range(steps):
        state_load(i).wait()
        for b in range(i * SEQ_STEP, (i + 1) * SEQ_STEP, 2):
            pair = jnp.concatenate(
                [jnp.where(row_of == b + n, u_vec, 0.0) for n in range(2)], axis=1
            ).astype(bf16)
            outer = dot(written, pair)
            old = [
                jnp.concatenate([state[b + n, h].astype(bf16) for h in range(heads)], axis=0)
                for n in range(2)
            ]
            read = dot_rows(jnp.concatenate(old, axis=1), readers)
            if b:
                read = jnp.where((lane_of == b) | (lane_of == count + b + 1), read, mixed[...])
            mixed[...] = read
            for n in range(2):
                for h in range(heads):
                    fade = decays[b + n : b + n + 1, h * n_state : (h + 1) * n_state]
                    state[b + n, h] = (
                        state[b + n, h] * fade
                        + outer[h * head_dim : (h + 1) * head_dim, n * n_state : (n + 1) * n_state]
                    )
        state_store(i).start()

    read = mixed[...].T
    even = lax.rem(lax.broadcasted_iota(jnp.int32, (count, inner), 0), 2) == 0
    read = jnp.where(even, read[:count], read[count:])
    mixed_out = decay_wide * read + moved * jnp.sum(u_vec * c_vec, axis=1, keepdims=True)
    skip_wide = jnp.concatenate(
        [jnp.broadcast_to(skip[:, h : h + 1], (1, head_dim)) for h in range(heads)], axis=1
    )
    gated = (mixed_out + skip_wide * inner_conv) * silu(gate_pre)
    squares = jnp.mean(gated * gated, axis=-1, keepdims=True)
    rows_out[...] = (gated * lax.rsqrt(squares + eps) * ggain[...]).astype(bf16)
    for i in range(steps):
        state_store(i).wait()
    for copy in win_copies:
        copy.wait()


def padded(rows):
    return -(-rows // 16) * 16


def flipped(a, b):
    low = lax.rem(a + b, 2)
    high = lax.rem(a // 2 + b // 2, 2)
    return 2 * high + low


def flip(index, mask):
    moved = index
    bit = 1
    while bit <= mask:
        if mask & bit:
            moved = moved + bit * (1 - 2 * lax.rem(index // bit, 2))
        bit *= 2
    return moved


def branches(
    ep_size,
    tp_size,
    slice_rows,
    chunks,
    mrows,
    outw,
    tokens,
    gain,
    routes,
    rweights,
    scale,
    gate_hbm,
    up_hbm,
    down_hbm,
    dgate_hbm,
    dup_hbm,
    ddown_hbm,
    out,
    scales,
    weights_in,
    down_w,
    dense_w,
    table_send,
    tables,
    part,
    parts,
    residual,
    rows,
    flat,
    pre,
    act,
    hid,
    shares,
    y_part,
    y_recv,
    z_send,
    z_recv,
    near_sems,
    load_sems,
    part_sems,
    table_sems,
    scale_sems,
    dense_sems,
    row_send,
    row_sems,
    relay_send,
    relay_sems,
    y_sems,
    z_sems,
):
    f32 = jnp.float32
    bf16 = jnp.bfloat16
    me_e = lax.axis_index("ep")
    me_t = lax.axis_index("tp")
    side = me_t // 2
    core = lax.rem(me_t, 2)
    partner = flip(me_t, 1)
    count, width = tokens.shape
    own_width = width // tp_size
    hidden_width = dgate_hbm.shape[0]
    halves = tp_size // 2
    expert_hidden = gate_hbm.shape[1]
    dense_at = [2 * expert_hidden, 2 * expert_hidden + padded(slice_rows)]

    def remote(src, dst, send, recv, to_e, to_t):
        copy = pltpu.make_async_remote_copy(
            src_ref=src,
            dst_ref=dst,
            send_sem=send,
            recv_sem=recv,
            device_id=(to_e, to_t),
            device_id_type=pl.DeviceIdType.MESH,
        )
        copy.start()
        return copy

    def settle(ref, sem):
        pltpu.make_async_copy(ref, ref, sem).wait()

    def tell(sem, to_e, to_t):
        pl.semaphore_signal(
            sem, inc=1, device_id=(to_e, to_t), device_id_type=pl.DeviceIdType.MESH
        )

    barrier = pltpu.get_barrier_semaphore()
    staged = ep_size == 8
    line = me_e // 2
    last = ep_size // 2 - 1

    def tell_line(sem, distance, to_t):
        pl.when(line >= distance)(lambda: tell(sem, me_e - 2 * distance, to_t))
        pl.when(line + distance <= last)(lambda: tell(sem, me_e + 2 * distance, to_t))

    def line_peers(distance):
        below = jnp.where(line >= distance, 1, 0)
        return below + jnp.where(line + distance <= last, 1, 0)

    for m in range(1, tp_size):
        tell(barrier, me_e, flip(me_t, m))
    if staged:
        tell(barrier, flip(me_e, 1), me_t)
        tell_line(barrier, 1, me_t)
    else:
        for m in range(ep_size - 1, 0, -1):
            tell(barrier, flip(me_e, m), partner)

    def dense_rows(ref, t):
        if slice_rows == hidden_width:
            return ref
        return ref.at[pl.ds(t * slice_rows, slice_rows)]

    dense_hbm = [dgate_hbm, dup_hbm, ddown_hbm]
    for src, dst, sem in [
        (gate_hbm.at[0], weights_in.at[pl.ds(0, expert_hidden)], 0),
        (up_hbm.at[0], weights_in.at[pl.ds(expert_hidden, expert_hidden)], 0),
        (down_hbm.at[0], down_w, 1),
    ] + [(dense_rows(dense_hbm[k], me_t), dense_w.at[0, k], 2) for k in range(3)]:
        pltpu.make_async_copy(src, dst, load_sems.at[sem]).start()

    mixer_rows = mrows[...]
    for q in range(tp_size):
        piece = dot(mixer_rows, outw[:, q * own_width : (q + 1) * own_width])
        part[q % 2, q // 2] = piece.astype(bf16)
    expert_of = lax.broadcasted_iota(jnp.int32, (ep_size, count), 0)
    table = jnp.zeros((ep_size, count), f32)
    for k in range(routes.shape[0]):
        table = table + jnp.where(expert_of == routes[k : k + 1, :], rweights[k : k + 1, :], 0.0)
    table = jnp.concatenate([table, jnp.zeros((ep_size, LANES - count), f32)], axis=1)
    for m in range(ep_size):
        table_send[m] = table[m : m + 1]
    tables[me_e] = table_send[me_e]
    scales[0] = scale[...]

    if staged:
        pl.semaphore_wait(barrier, tp_size + line_peers(1))
        tell_line(near_sems.at[0], 1, me_t)
    else:
        pl.semaphore_wait(barrier, ep_size + tp_size - 2)
    tp_order = [m for m in range(2, tp_size)] + [1]
    for m in tp_order:
        to = flip(me_t, m)
        remote(
            part.at[lax.rem(to, 2)], parts.at[m], part_sems.at[0], part_sems.at[1], me_e, to
        )
    for m in tp_order:
        to = flip(me_t, m)
        remote(scales.at[0], scales.at[m], scale_sems.at[0], scale_sems.at[1], me_e, to)
        for k in range(3):
            remote(
                dense_rows(dense_hbm[k], to),
                dense_w.at[m, k],
                dense_sems.at[0],
                dense_sems.at[1],
                me_e,
                to,
            )

    if staged:
        pl.semaphore_wait(near_sems.at[0], line_peers(1))
        tell_line(near_sems.at[1], 1, me_t)
        tell_line(near_sems.at[1], 2, me_t)
        pl.semaphore_wait(near_sems.at[1], line_peers(1) + line_peers(2))
        tell(near_sems.at[2], me_e, partner)
    own_rows = []
    for h in range(halves):
        at = pl.ds(pl.multiple_of(core * own_width + 2 * h * own_width, own_width), own_width)
        own_rows.append(tokens[:, at].astype(f32) + part[core, h].astype(f32))
    settle(parts.at[pl.ds(1, tp_size - 1)], part_sems.at[1])
    for h in range(halves):
        for m in range(1, tp_size):
            own_rows[h] = own_rows[h] + parts[m, h].astype(f32)
        residual[h] = own_rows[h]
        rows[core, me_e, h] = own_rows[h].astype(bf16)

    if staged:
        pl.semaphore_wait(near_sems.at[2], 1)
    for m in range(ep_size - 1, 0, -1):
        remote(
            rows.at[core, me_e],
            rows.at[core, me_e],
            row_send.at[0],
            row_sems.at[me_e],
            flip(me_e, m),
            partner,
        )
    for m in range(1, ep_size):
        remote(
            table_send.at[flip(me_e, m)],
            tables.at[me_e],
            table_sems.at[0],
            table_sems.at[1],
            flip(me_e, m),
            partner,
        )

    def block_of(chunk, place):
        start, length = chunk
        return start + flip(lax.rem(me_e, length), place)

    def is_home(chunk):
        start, length = chunk
        return me_e // length == start // length

    def relay(chunk, place):
        m = block_of(chunk, place)

        def pass_on(half):
            remote(
                rows.at[half, m],
                rows.at[half, m],
                relay_send.at[0],
                relay_sems.at[m],
                me_e,
                partner,
            )

        def forward():
            settle(rows.at[1 - core, m], row_sems.at[m])
            pass_on(1 - core)

        if place:
            forward()
        else:
            home = is_home(chunk)
            pl.when(home)(lambda: pass_on(core))
            pl.when(jnp.logical_not(home))(forward)

    def normalize(chunk, places):
        blocks = [(at, block_of(chunk, at)) for at in places]
        for at, m in blocks:
            settle(rows.at[core, m], relay_sems.at[m])
        for at, m in blocks:
            pieces = [rows[q % 2, m, q // 2].astype(f32) for q in range(tp_size)]
            squares = pieces[0] * pieces[0]
            for q in range(1, tp_size):
                squares = squares + pieces[q] * pieces[q]
            scale_of = lax.rsqrt(jnp.sum(squares, axis=-1, keepdims=True) * (1.0 / width) + eps)
            for q in range(tp_size):
                lanes = slice(q * own_width, (q + 1) * own_width)
                flat[at * count : (at + 1) * count, lanes] = pieces[q] * scale_of * gain[:, lanes]

    unit = LANES
    if slice_rows == hidden_width:
        units = lax.broadcasted_iota(jnp.int32, (slice_rows, 1), 0)
        share = hidden_width // tp_size
        kept = (units // share == me_t).astype(f32)

    def weigh(m):
        row = tables[m][:, :count]
        diagonal = lax.broadcasted_iota(jnp.int32, (count, count), 0) == lax.broadcasted_iota(
            jnp.int32, (count, count), 1
        )
        weight = jnp.sum(jnp.where(diagonal, row, 0.0), axis=1, keepdims=True)
        shares[m] = jnp.broadcast_to(weight, (count, own_width))

    def place_weights():
        settle(weights_in.at[pl.ds(0, 2 * expert_hidden)], load_sems.at[0])
        settle(down_w, load_sems.at[1])
        settle(dense_w.at[0], load_sems.at[2])
        settle(tables.at[pl.ds(0, ep_size - 1)], table_sems.at[1])
        settle(scales.at[pl.ds(1, tp_size - 1)], scale_sems.at[1])
        settle(dense_w.at[pl.ds(1, tp_size - 1)], dense_sems.at[1])
        for k in range(2):
            at = slice(dense_at[k], dense_at[k] + slice_rows)
            for m in range(tp_size):
                lanes = pl.ds(pl.multiple_of(flip(me_t, m) * own_width, own_width), own_width)
                weights_in[at, lanes] = dense_w[m, k]
        for m in range(ep_size):
            weigh(m)

    def activate(chunk):
        live = chunk[1] * count
        lanes = slice(0, live)
        x = flat[:live, :].astype(bf16)
        pre[:, lanes] = dot_rows(weights_in[...], x)
        for n in range(0, expert_hidden, unit):
            end = min(n + unit, expert_hidden)
            gate_act = pre[n:end, lanes]
            up_act = pre[expert_hidden + n : expert_hidden + end, lanes]
            act[lanes, n:end] = (silu(gate_act) * up_act).T.astype(bf16)
        gate_act = pre[dense_at[0] : dense_at[0] + slice_rows, lanes]
        up_act = pre[dense_at[1] : dense_at[1] + slice_rows, lanes]
        hidden = silu(gate_act) * up_act
        if slice_rows == hidden_width:
            hidden = hidden * kept
        hid[:, lanes] = hidden.astype(bf16)

    contract_rows = (((0,), (0,)), ((), ()))

    def project(chunk, first):
        live = chunk[1] * count
        weights = [shares[block_of(chunk, g)] for g in range(chunk[1])]
        acts = act[:live, :]
        hidden = hid[:, :live]
        for mine in range(2):
            whose = 1 - core if mine else core
            for h in range(halves):
                t = 2 * h + whose
                lanes = pl.ds(pl.multiple_of(t * own_width, own_width), own_width)
                slot = flipped(me_t, t)
                routed = dot(acts, down_w[:, lanes])
                dense = lax.dot_general(
                    hidden, dense_w[slot, 2], contract_rows, preferred_element_type=f32
                )
                for g in range(chunk[1]):
                    at = slice(g * count, (g + 1) * count)
                    y = routed[at] * weights[g] + dense[at] * scales[slot]
                    y_part[mine, h, first + g] = y.astype(bf16)
                if not mine:
                    at = pl.ds(first, chunk[1])
                    y_copies.append(
                        remote(
                            y_part.at[0, h, at],
                            y_recv.at[h, at],
                            y_sems.at[0, len(y_copies)],
                            y_sems.at[1, len(y_copies)],
                            me_e,
                            partner,
                        )
                    )
    def give_back(chunk, first, sent):
        for to_side in range(halves):
            sent[to_side].wait_recv()
            for g in range(chunk[1] - 1, -1, -1):
                m = block_of(chunk, g)
                at = to_side * ep_size + first + g
                summed = y_part[1, to_side, first + g].astype(f32)
                summed = summed + y_recv[to_side, first + g].astype(f32)

                z_send[at] = summed.astype(bf16)
                remote(
                    z_send.at[at],
                    z_recv.at[side * ep_size + me_e],
                    z_sems.at[0],
                    z_sems.at[1],
                    m,
                    2 * to_side + 1 - core,
                )

    y_copies = []
    for k, chunk in enumerate(chunks):
        late = max(chunk[1] - RELAY_LAG, 0)
        for place in range(chunk[1]):
            relay(chunk, place)
            if place >= RELAY_LAG:
                normalize(chunk, [place - RELAY_LAG])
        if k == 0:
            place_weights()
        normalize(chunk, range(late, chunk[1]))
        activate(chunk)
        project(chunk, chunk[0])
        give_back(chunk, chunk[0], y_copies[halves * k :])

    settle(z_recv, z_sems.at[1])
    final = residual[side]
    for m in range(halves * ep_size):
        final = final + z_recv[m].astype(f32)
    out[...] = final.astype(bf16)

    settle(parts.at[pl.ds(1, tp_size - 1)], part_sems.at[0])
    settle(tables.at[pl.ds(0, ep_size - 1)], table_sems.at[0])
    settle(scales.at[pl.ds(1, tp_size - 1)], scale_sems.at[0])
    settle(dense_w.at[pl.ds(1, tp_size - 1)], dense_sems.at[0])
    settle(rows.at[0, pl.ds(1, ep_size - 1)], row_send.at[0])
    settle(rows.at[0], relay_send.at[0])
    for copy in y_copies:
        copy.wait_send()
    settle(z_send, z_sems.at[0])


def local(
    tokens,
    mixer_gain,
    gate_weight,
    inner_weight,
    state_weight,
    step_weight,
    step_bias,
    decay_log,
    skip_scale,
    inner_kernel,
    state_kernel,
    inner_window,
    state_window,
    recurrent_state,
    group_gain,
    output_weight,
    channel_gain,
    routes,
    route_weights,
    expert_gate,
    expert_up,
    expert_down,
    dense_gate,
    dense_up,
    dense_down,
    dense_scale,
):
    f32 = jnp.float32
    bf16 = jnp.bfloat16
    ep_size = lax.axis_size("ep")
    tp_size = lax.axis_size("tp")
    count, width = tokens.shape
    own_width = width // tp_size
    hbm = pl.BlockSpec(memory_space=pltpu.HBM)
    on_chip = pl.BlockSpec(memory_space=pltpu.VMEM)
    dma = pltpu.SemaphoreType.DMA
    vmem = pltpu.VMEM
    steps = count // SEQ_STEP

    inner_window = jnp.swapaxes(inner_window, 0, 1)
    taps = inner_kernel.shape[0]
    inner = inner_weight.shape[1]
    mixer_args = [
        tokens,
        mixer_gain[None],
        gate_weight,
        inner_weight,
        state_weight,
        step_weight.T,
        step_bias[None],
        decay_log[None],
        skip_scale[None],
        inner_kernel,
        state_kernel,
        inner_window,
        state_window,
        recurrent_state,
        group_gain[None],
    ]
    held = [vmem(a.shape, a.dtype) for a in mixer_args]
    held[11] = vmem((taps,) + inner_window.shape[1:], bf16)
    held[12] = vmem((count, taps) + state_window.shape[2:], bf16)
    heads = step_bias.shape[0]
    n_state = state_weight.shape[2]
    mixer_rows, new_state, new_inner, new_state_window = pl.pallas_call(
        mixer,
        out_shape=[
            jax.ShapeDtypeStruct((count, inner), bf16),
            jax.ShapeDtypeStruct(recurrent_state.shape, f32),
            jax.ShapeDtypeStruct(inner_window.shape, bf16),
            jax.ShapeDtypeStruct(state_window.shape, bf16),
        ],
        in_specs=[hbm] * len(mixer_args),
        out_specs=[on_chip] + [hbm] * 3,
        scratch_shapes=held
        + [
            vmem((count, heads * n_state), f32),
            vmem((inner, 2 * count), f32),
            dma((14,)),
            dma((2, steps)),
            dma((2,)),
        ],
        compiler_params=pltpu.CompilerParams(vmem_limit_bytes=24 * 1024 * 1024),
    )(*[pltpu.with_memory_space_constraint(a, pltpu.HBM) for a in mixer_args])

    expert_gate = jnp.swapaxes(expert_gate, 1, 2)
    expert_up = jnp.swapaxes(expert_up, 1, 2)
    hidden_width = dense_gate.shape[1]
    expert_hidden = expert_gate.shape[1]
    slice_rows = hidden_width // tp_size
    if hidden_width % (8 * tp_size):
        slice_rows = hidden_width
    halves = tp_size // 2
    chunks = CHUNKS if ep_size == 8 else [(k, 8) for k in range(0, ep_size, 8)]
    live = max(length for _, length in chunks) * count
    wide = 2 * (expert_hidden + padded(slice_rows))
    branch_args = [
        mixer_rows,
        output_weight,
        tokens,
        channel_gain[None],
        routes.T,
        route_weights.T,
        dense_scale[None],
        expert_gate,
        expert_up,
        expert_down,
        dense_gate.T,
        dense_up.T,
        dense_down,
    ]
    new_tokens = pl.pallas_call(
        functools.partial(branches, ep_size, tp_size, slice_rows, chunks),
        out_shape=jax.ShapeDtypeStruct((count, own_width), bf16),
        in_specs=[on_chip] * 7 + [hbm] * (len(branch_args) - 7),
        out_specs=pl.BlockSpec(memory_space=pltpu.VMEM),
        scratch_shapes=[
            vmem((tp_size, 1, own_width), f32),
            vmem((wide, width), bf16),
            vmem(expert_down.shape[1:], bf16),
            vmem((tp_size, 3, slice_rows, own_width), bf16),
            vmem((ep_size, 1, LANES), f32),
            vmem((ep_size, 1, LANES), f32),
            vmem((2, halves, count, own_width), bf16),
            vmem((tp_size, halves, count, own_width), bf16),
            vmem((halves, count, own_width), f32),
            vmem((2, ep_size, halves, count, own_width), bf16),
            vmem((live, width), f32),
            vmem((wide, live), f32),
            vmem((live, expert_hidden), bf16),
            vmem((slice_rows, live), bf16),
            vmem((ep_size, count, own_width), f32),
            vmem((2, halves, ep_size, count, own_width), bf16),
            vmem((halves, ep_size, count, own_width), bf16),
            vmem((halves * ep_size, count, own_width), bf16),
            vmem((halves * ep_size, count, own_width), bf16),
            pltpu.SemaphoreType.REGULAR((3,)),
            dma((3,)),
            dma((2,)),
            dma((2,)),
            dma((2,)),
            dma((2,)),
            dma((1,)),
            dma((ep_size,)),
            dma((1,)),
            dma((ep_size,)),
            dma((2, halves * len(chunks))),
            dma((2,)),
        ],
        compiler_params=pltpu.CompilerParams(
            collective_id=0, has_side_effects=True, vmem_limit_bytes=(24 if ep_size <= 8 else 56) * 1024 * 1024
        ),
    )(*branch_args[:7], *[pltpu.with_memory_space_constraint(a, pltpu.HBM) for a in branch_args[7:]])
    return (
        new_tokens,
        new_state,
        jnp.swapaxes(new_inner, 0, 1),
        new_state_window,
    )


def solution(mesh):
    placed = (
        P("ep", None),
        P(),
        P(None, "tp"),
        P(None, "tp"),
        P(None, None, "tp"),
        P(None, "tp"),
        P("tp"),
        P("tp"),
        P("tp"),
        P(None, "tp"),
        P(None, None, "tp"),
        P("ep", None, "tp"),
        P("ep", None, None, "tp"),
        P("ep", "tp", None, None),
        P("tp"),
        P("tp", None),
        P(),
        P("ep", None),
        P("ep", None),
        P("ep", None, "tp"),
        P("ep", None, "tp"),
        P("ep", "tp", None),
        P("tp", "ep"),
        P("tp", "ep"),
        P("ep", "tp"),
        P("tp"),
    )
    return jax.shard_map(
        local,
        mesh=mesh,
        in_specs=placed,
        out_specs=(
            P("ep", "tp"),
            P("ep", "tp", None, None),
            P("ep", None, "tp"),
            P("ep", None, None, "tp"),
        ),
        check_vma=False,
    )
```

```python
import functools

import jax
import jax.numpy as jnp
from jax import lax
from jax.experimental import pallas as pl
from jax.experimental.pallas import tpu as pltpu
from jax.sharding import PartitionSpec as P

HEADS = 16
GROUPS = 4
HEAD_DIM = 64
STATE_DIM = 128
LANES = 128
SEQ_STEP = 6
DEST_ORDER = (0, 1, 7, 6, 5, 4, 3, 2)
RELAY_LAG = 8
CHUNKS = ((0, 8),)

eps = 1e-06


def silu(v):
    return v / (1.0 + jnp.exp(-v))


def dot_rows(rows, columns):
    return lax.dot_general(
        rows, columns, (((1,), (1,)), ((), ())), preferred_element_type=jnp.float32
    )


def dot(a, b):
    return jnp.dot(a, b, preferred_element_type=jnp.float32)


def mixer(
    tokens_hbm,
    mgain_hbm,
    gatew_hbm,
    innerw_hbm,
    statew_hbm,
    stepw_hbm,
    sbias_hbm,
    dlog_hbm,
    skip_hbm,
    ikern_hbm,
    skern_hbm,
    iwin_hbm,
    swin_hbm,
    state_hbm,
    ggain_hbm,
    rows_out,
    state_out,
    iwin_out,
    swin_out,
    tokens,
    mgain,
    gatew,
    innerw,
    statew,
    stepw,
    sbias,
    dlog,
    skip,
    ikern,
    skern,
    iwin,
    swin,
    state,
    ggain,
    decays,
    mixed,
    sems,
    state_sems,
    out_sems,
):
    f32 = jnp.float32
    bf16 = jnp.bfloat16
    count = tokens.shape[0]
    taps = ikern.shape[0]
    heads = sbias.shape[1]
    inner = innerw.shape[1]
    head_dim = inner // heads
    n_state = statew.shape[2]
    small = [
        (tokens_hbm, tokens),
        (mgain_hbm, mgain),
        (innerw_hbm, innerw),
        (statew_hbm, statew),
        (stepw_hbm, stepw),
        (sbias_hbm, sbias),
        (dlog_hbm, dlog),
        (ikern_hbm, ikern),
        (skern_hbm, skern),
        (iwin_hbm, iwin.at[pl.ds(0, taps - 1)]),
        (swin_hbm, swin.at[:, pl.ds(0, taps - 1)]),
        (gatew_hbm, gatew),
        (skip_hbm, skip),
        (ggain_hbm, ggain),
    ]
    loads = []
    for i, (src, dst) in enumerate(small):
        copy = pltpu.make_async_copy(src, dst, sems.at[i])
        copy.start()
        loads.append(copy)

    def state_load(i):
        at = pl.ds(i * SEQ_STEP, SEQ_STEP)
        return pltpu.make_async_copy(state_hbm.at[at], state.at[at], state_sems.at[0, i])

    def state_store(i):
        at = pl.ds(i * SEQ_STEP, SEQ_STEP)
        return pltpu.make_async_copy(state.at[at], state_out.at[at], state_sems.at[1, i])

    steps = count // SEQ_STEP
    loads[0].wait()
    loads[1].wait()
    for i in range(steps):
        state_load(i).start()
    value = tokens[...].astype(f32)
    squares = jnp.mean(value * value, axis=-1, keepdims=True)
    normed = (value * lax.rsqrt(squares + eps) * mgain[...]).astype(bf16)
    for i in range(2, 14):
        loads[i].wait()
    inner_pre = dot(normed, innerw[...]).astype(bf16)
    pre_u = dot(normed, statew[0])
    pre_c = dot(normed, statew[1])
    step_raw = dot_rows(normed, stepw[...])
    gate_pre = dot(normed, gatew[...])

    iwin[taps - 1] = inner_pre
    conv = inner_pre.astype(f32) * ikern[taps - 1 : taps, :]
    for j in range(taps - 1):
        conv = conv + iwin[j].astype(f32) * ikern[j : j + 1, :]
    inner_conv = silu(conv)

    both = jnp.concatenate([pre_u[:, None, :], pre_c[:, None, :]], axis=1).astype(bf16)
    swin[:, taps - 1] = both
    sconv = both.astype(f32) * skern[taps - 1][None]
    for j in range(taps - 1):
        sconv = sconv + swin[:, j].astype(f32) * skern[j][None]
    sconv = silu(sconv)
    u_vec = sconv[:, 0, :]
    c_vec = sconv[:, 1, :]
    win_copies = [
        pltpu.make_async_copy(iwin.at[pl.ds(1, taps - 1)], iwin_out, out_sems.at[0]),
        pltpu.make_async_copy(swin.at[:, pl.ds(1, taps - 1)], swin_out, out_sems.at[1]),
    ]
    for copy in win_copies:
        copy.start()

    step_size = jax.nn.softplus(step_raw + sbias[...])
    decay = jnp.exp(-step_size * jnp.exp(dlog[...]))
    step_wide = jnp.concatenate(
        [jnp.broadcast_to(step_size[:, h : h + 1], (count, head_dim)) for h in range(heads)],
        axis=1,
    )
    decay_wide = jnp.concatenate(
        [jnp.broadcast_to(decay[:, h : h + 1], (count, head_dim)) for h in range(heads)], axis=1
    )
    for h in range(heads):
        decays[:, h * n_state : (h + 1) * n_state] = jnp.broadcast_to(
            decay[:, h : h + 1], (count, n_state)
        )
    moved = step_wide * inner_conv
    written = moved.T.astype(bf16)
    row_of = lax.broadcasted_iota(jnp.int32, (count, n_state), 0)
    lane_of = lax.broadcasted_iota(jnp.int32, (inner, 2 * count), 1)
    none = jnp.zeros_like(c_vec)
    readers = jnp.concatenate(
        [jnp.concatenate([c_vec, none], axis=1), jnp.concatenate([none, c_vec], axis=1)], axis=0
    ).astype(bf16)

    for i in range(steps):
        state_load(i).wait()
        for b in range(i * SEQ_STEP, (i + 1) * SEQ_STEP, 2):
            pair = jnp.concatenate(
                [jnp.where(row_of == b + n, u_vec, 0.0) for n in range(2)], axis=1
            ).astype(bf16)
            outer = dot(written, pair)
            old = [
                jnp.concatenate([state[b + n, h].astype(bf16) for h in range(heads)], axis=0)
                for n in range(2)
            ]
            read = dot_rows(jnp.concatenate(old, axis=1), readers)
            if b:
                read = jnp.where((lane_of == b) | (lane_of == count + b + 1), read, mixed[...])
            mixed[...] = read
            for n in range(2):
                for h in range(heads):
                    fade = decays[b + n : b + n + 1, h * n_state : (h + 1) * n_state]
                    state[b + n, h] = (
                        state[b + n, h] * fade
                        + outer[h * head_dim : (h + 1) * head_dim, n * n_state : (n + 1) * n_state]
                    )
        state_store(i).start()

    read = mixed[...].T
    even = lax.rem(lax.broadcasted_iota(jnp.int32, (count, inner), 0), 2) == 0
    read = jnp.where(even, read[:count], read[count:])
    mixed_out = decay_wide * read + moved * jnp.sum(u_vec * c_vec, axis=1, keepdims=True)
    skip_wide = jnp.concatenate(
        [jnp.broadcast_to(skip[:, h : h + 1], (1, head_dim)) for h in range(heads)], axis=1
    )
    gated = (mixed_out + skip_wide * inner_conv) * silu(gate_pre)
    squares = jnp.mean(gated * gated, axis=-1, keepdims=True)
    rows_out[...] = (gated * lax.rsqrt(squares + eps) * ggain[...]).astype(bf16)
    for i in range(steps):
        state_store(i).wait()
    for copy in win_copies:
        copy.wait()


def padded(rows):
    return -(-rows // 16) * 16


def flipped(a, b):
    low = lax.rem(a + b, 2)
    high = lax.rem(a // 2 + b // 2, 2)
    return 2 * high + low


def flip(index, mask):
    moved = index
    bit = 1
    while bit <= mask:
        if mask & bit:
            moved = moved + bit * (1 - 2 * lax.rem(index // bit, 2))
        bit *= 2
    return moved


def branches(
    ep_size,
    tp_size,
    slice_rows,
    chunks,
    mrows,
    outw,
    tokens,
    gain,
    routes,
    rweights,
    scale,
    gate_hbm,
    up_hbm,
    down_hbm,
    dgate_hbm,
    dup_hbm,
    ddown_hbm,
    out,
    scales,
    weights_in,
    down_w,
    dense_w,
    table_send,
    tables,
    part,
    parts,
    residual,
    rows,
    flat,
    pre,
    act,
    hid,
    shares,
    y_part,
    y_recv,
    z_send,
    z_recv,
    near_sems,
    load_sems,
    part_sems,
    table_sems,
    scale_sems,
    dense_sems,
    row_send,
    row_sems,
    relay_send,
    relay_sems,
    y_sems,
    z_sems,
):
    f32 = jnp.float32
    bf16 = jnp.bfloat16
    me_e = lax.axis_index("ep")
    me_t = lax.axis_index("tp")
    side = me_t // 2
    core = lax.rem(me_t, 2)
    partner = flip(me_t, 1)
    count, width = tokens.shape
    own_width = width // tp_size
    hidden_width = dgate_hbm.shape[0]
    halves = tp_size // 2
    expert_hidden = gate_hbm.shape[1]
    dense_at = [2 * expert_hidden, 2 * expert_hidden + padded(slice_rows)]

    def remote(src, dst, send, recv, to_e, to_t):
        copy = pltpu.make_async_remote_copy(
            src_ref=src,
            dst_ref=dst,
            send_sem=send,
            recv_sem=recv,
            device_id=(to_e, to_t),
            device_id_type=pl.DeviceIdType.MESH,
        )
        copy.start()
        return copy

    def settle(ref, sem):
        pltpu.make_async_copy(ref, ref, sem).wait()

    def tell(sem, to_e, to_t):
        pl.semaphore_signal(
            sem, inc=1, device_id=(to_e, to_t), device_id_type=pl.DeviceIdType.MESH
        )

    barrier = pltpu.get_barrier_semaphore()
    staged = ep_size == 8
    line = me_e // 2
    last = ep_size // 2 - 1

    def tell_line(sem, distance, to_t):
        pl.when(line >= distance)(lambda: tell(sem, me_e - 2 * distance, to_t))
        pl.when(line + distance <= last)(lambda: tell(sem, me_e + 2 * distance, to_t))

    def line_peers(distance):
        below = jnp.where(line >= distance, 1, 0)
        return below + jnp.where(line + distance <= last, 1, 0)

    for m in range(1, tp_size):
        tell(barrier, me_e, flip(me_t, m))
    if staged:
        tell(barrier, flip(me_e, 1), me_t)
        tell_line(barrier, 1, me_t)
    else:
        for m in range(ep_size - 1, 0, -1):
            tell(barrier, flip(me_e, m), partner)

    def dense_rows(ref, t):
        if slice_rows == hidden_width:
            return ref
        return ref.at[pl.ds(t * slice_rows, slice_rows)]

    dense_hbm = [dgate_hbm, dup_hbm, ddown_hbm]
    for src, dst, sem in [
        (gate_hbm.at[0], weights_in.at[pl.ds(0, expert_hidden)], 0),
        (up_hbm.at[0], weights_in.at[pl.ds(expert_hidden, expert_hidden)], 0),
        (down_hbm.at[0], down_w, 1),
    ] + [(dense_rows(dense_hbm[k], me_t), dense_w.at[0, k], 2) for k in range(3)]:
        pltpu.make_async_copy(src, dst, load_sems.at[sem]).start()

    mixer_rows = mrows[...]
    for q in range(tp_size):
        piece = dot(mixer_rows, outw[:, q * own_width : (q + 1) * own_width])
        part[q % 2, q // 2] = piece.astype(bf16)
    scales[0] = scale[...]

    if staged:
        pl.semaphore_wait(barrier, tp_size + line_peers(1))
        tell_line(near_sems.at[0], 1, me_t)
    else:
        pl.semaphore_wait(barrier, ep_size + tp_size - 2)
    tp_order = [m for m in range(2, tp_size)] + [1]
    for m in tp_order:
        to = flip(me_t, m)
        remote(
            part.at[lax.rem(to, 2)], parts.at[m], part_sems.at[0], part_sems.at[1], me_e, to
        )
    for m in tp_order:
        to = flip(me_t, m)
        remote(scales.at[0], scales.at[m], scale_sems.at[0], scale_sems.at[1], me_e, to)
        for k in range(3):
            remote(
                dense_rows(dense_hbm[k], to),
                dense_w.at[m, k],
                dense_sems.at[0],
                dense_sems.at[1],
                me_e,
                to,
            )

    expert_of = lax.broadcasted_iota(jnp.int32, (ep_size, count), 0)
    table = jnp.zeros((ep_size, count), f32)
    for k in range(routes.shape[0]):
        table = table + jnp.where(expert_of == routes[k : k + 1, :], rweights[k : k + 1, :], 0.0)
    table = jnp.concatenate([table, jnp.zeros((ep_size, LANES - count), f32)], axis=1)
    for m in range(ep_size):
        table_send[m] = table[m : m + 1]
    tables[me_e] = table_send[me_e]
    if staged:
        pl.semaphore_wait(near_sems.at[0], line_peers(1))
        tell_line(near_sems.at[1], 1, me_t)
        tell_line(near_sems.at[1], 2, me_t)
        pl.semaphore_wait(near_sems.at[1], line_peers(1) + line_peers(2))
        tell(near_sems.at[2], me_e, partner)
    own_rows = []
    for h in range(halves):
        at = pl.ds(pl.multiple_of(core * own_width + 2 * h * own_width, own_width), own_width)
        own_rows.append(tokens[:, at].astype(f32) + part[core, h].astype(f32))
    settle(parts.at[pl.ds(1, tp_size - 1)], part_sems.at[1])
    for h in range(halves):
        for m in range(1, tp_size):
            own_rows[h] = own_rows[h] + parts[m, h].astype(f32)
        residual[h] = own_rows[h]
        rows[core, me_e, h] = own_rows[h].astype(bf16)

    if staged:
        pl.semaphore_wait(near_sems.at[2], 1)
    for m in range(ep_size - 1, 0, -1):
        remote(
            rows.at[core, me_e],
            rows.at[core, me_e],
            row_send.at[0],
            row_sems.at[me_e],
            flip(me_e, m),
            partner,
        )
    for m in range(1, ep_size):
        remote(
            table_send.at[flip(me_e, m)],
            tables.at[me_e],
            table_sems.at[0],
            table_sems.at[1],
            flip(me_e, m),
            partner,
        )

    def block_of(chunk, place):
        start, length = chunk
        return start + flip(lax.rem(me_e, length), place)

    def is_home(chunk):
        start, length = chunk
        return me_e // length == start // length

    def relay(chunk, place):
        m = block_of(chunk, place)

        def pass_on(half):
            remote(
                rows.at[half, m],
                rows.at[half, m],
                relay_send.at[0],
                relay_sems.at[m],
                me_e,
                partner,
            )

        def forward():
            settle(rows.at[1 - core, m], row_sems.at[m])
            pass_on(1 - core)

        if place:
            forward()
        else:
            home = is_home(chunk)
            pl.when(home)(lambda: pass_on(core))
            pl.when(jnp.logical_not(home))(forward)

    def normalize(chunk, places):
        blocks = [(at, block_of(chunk, at)) for at in places]
        for at, m in blocks:
            settle(rows.at[core, m], relay_sems.at[m])
        for at, m in blocks:
            pieces = [rows[q % 2, m, q // 2].astype(f32) for q in range(tp_size)]
            squares = pieces[0] * pieces[0]
            for q in range(1, tp_size):
                squares = squares + pieces[q] * pieces[q]
            scale_of = lax.rsqrt(jnp.sum(squares, axis=-1, keepdims=True) * (1.0 / width) + eps)
            for q in range(tp_size):
                lanes = slice(q * own_width, (q + 1) * own_width)
                flat[at * count : (at + 1) * count, lanes] = pieces[q] * scale_of * gain[:, lanes]

    unit = LANES
    if slice_rows == hidden_width:
        units = lax.broadcasted_iota(jnp.int32, (slice_rows, 1), 0)
        share = hidden_width // tp_size
        kept = (units // share == me_t).astype(f32)

    def weigh(m):
        row = tables[m][:, :count]
        diagonal = lax.broadcasted_iota(jnp.int32, (count, count), 0) == lax.broadcasted_iota(
            jnp.int32, (count, count), 1
        )
        weight = jnp.sum(jnp.where(diagonal, row, 0.0), axis=1, keepdims=True)
        shares[m] = jnp.broadcast_to(weight, (count, own_width))

    def place_weights():
        settle(weights_in.at[pl.ds(0, 2 * expert_hidden)], load_sems.at[0])
        settle(down_w, load_sems.at[1])
        settle(dense_w.at[0], load_sems.at[2])
        settle(tables.at[pl.ds(0, ep_size - 1)], table_sems.at[1])
        settle(scales.at[pl.ds(1, tp_size - 1)], scale_sems.at[1])
        settle(dense_w.at[pl.ds(1, tp_size - 1)], dense_sems.at[1])
        for k in range(2):
            at = slice(dense_at[k], dense_at[k] + slice_rows)
            for m in range(tp_size):
                lanes = pl.ds(pl.multiple_of(flip(me_t, m) * own_width, own_width), own_width)
                weights_in[at, lanes] = dense_w[m, k]
        for m in range(ep_size):
            weigh(m)

    def activate(chunk):
        live = chunk[1] * count
        lanes = slice(0, live)
        x = flat[:live, :].astype(bf16)
        pre[:, lanes] = dot_rows(weights_in[...], x)
        for n in range(0, expert_hidden, unit):
            end = min(n + unit, expert_hidden)
            gate_act = pre[n:end, lanes]
            up_act = pre[expert_hidden + n : expert_hidden + end, lanes]
            act[lanes, n:end] = (silu(gate_act) * up_act).T.astype(bf16)
        gate_act = pre[dense_at[0] : dense_at[0] + slice_rows, lanes]
        up_act = pre[dense_at[1] : dense_at[1] + slice_rows, lanes]
        hidden = silu(gate_act) * up_act
        if slice_rows == hidden_width:
            hidden = hidden * kept
        hid[:, lanes] = hidden.astype(bf16)

    contract_rows = (((0,), (0,)), ((), ()))

    def project(chunk, first):
        live = chunk[1] * count
        weights = [shares[block_of(chunk, g)] for g in range(chunk[1])]
        acts = act[:live, :]
        hidden = hid[:, :live]
        for mine in range(2):
            whose = 1 - core if mine else core
            for h in range(halves):
                t = 2 * h + whose
                lanes = pl.ds(pl.multiple_of(t * own_width, own_width), own_width)
                slot = flipped(me_t, t)
                routed = dot(acts, down_w[:, lanes])
                dense = lax.dot_general(
                    hidden, dense_w[slot, 2], contract_rows, preferred_element_type=f32
                )
                for g in range(chunk[1]):
                    at = slice(g * count, (g + 1) * count)
                    y = routed[at] * weights[g] + dense[at] * scales[slot]
                    y_part[mine, h, first + g] = y.astype(bf16)
                if not mine:
                    at = pl.ds(first, chunk[1])
                    y_copies.append(
                        remote(
                            y_part.at[0, h, at],
                            y_recv.at[h, at],
                            y_sems.at[0, len(y_copies)],
                            y_sems.at[1, len(y_copies)],
                            me_e,
                            partner,
                        )
                    )
    def give_back(chunk, first, sent):
        for to_side in range(halves):
            sent[to_side].wait_recv()
            for n in range(chunk[1]):
                if ep_size == 8:
                    m = DEST_ORDER[n]
                    place = flip(me_e, m)
                else:
                    place = first + chunk[1] - 1 - n
                    m = block_of(chunk, chunk[1] - 1 - n)
                at = to_side * ep_size + place
                summed = y_part[1, to_side, place].astype(f32)
                summed = summed + y_recv[to_side, place].astype(f32)
                z_send[at] = summed.astype(bf16)
                remote(
                    z_send.at[at],
                    z_recv.at[side * ep_size + me_e],
                    z_sems.at[0],
                    z_sems.at[1],
                    m,
                    2 * to_side + 1 - core,
                )

    y_copies = []
    for k, chunk in enumerate(chunks):
        late = max(chunk[1] - RELAY_LAG, 0)
        for place in range(chunk[1]):
            relay(chunk, place)
            if place >= RELAY_LAG:
                normalize(chunk, [place - RELAY_LAG])
        if k == 0:
            place_weights()
        normalize(chunk, range(late, chunk[1]))
        activate(chunk)
        project(chunk, chunk[0])
        give_back(chunk, chunk[0], y_copies[halves * k :])

    settle(z_recv, z_sems.at[1])
    final = residual[side]
    for m in range(halves * ep_size):
        final = final + z_recv[m].astype(f32)
    out[...] = final.astype(bf16)

    settle(parts.at[pl.ds(1, tp_size - 1)], part_sems.at[0])
    settle(tables.at[pl.ds(0, ep_size - 1)], table_sems.at[0])
    settle(scales.at[pl.ds(1, tp_size - 1)], scale_sems.at[0])
    settle(dense_w.at[pl.ds(1, tp_size - 1)], dense_sems.at[0])
    settle(rows.at[0, pl.ds(1, ep_size - 1)], row_send.at[0])
    settle(rows.at[0], relay_send.at[0])
    for copy in y_copies:
        copy.wait_send()
    settle(z_send, z_sems.at[0])


def local(
    tokens,
    mixer_gain,
    gate_weight,
    inner_weight,
    state_weight,
    step_weight,
    step_bias,
    decay_log,
    skip_scale,
    inner_kernel,
    state_kernel,
    inner_window,
    state_window,
    recurrent_state,
    group_gain,
    output_weight,
    channel_gain,
    routes,
    route_weights,
    expert_gate,
    expert_up,
    expert_down,
    dense_gate,
    dense_up,
    dense_down,
    dense_scale,
):
    f32 = jnp.float32
    bf16 = jnp.bfloat16
    ep_size = lax.axis_size("ep")
    tp_size = lax.axis_size("tp")
    count, width = tokens.shape
    own_width = width // tp_size
    hbm = pl.BlockSpec(memory_space=pltpu.HBM)
    on_chip = pl.BlockSpec(memory_space=pltpu.VMEM)
    dma = pltpu.SemaphoreType.DMA
    vmem = pltpu.VMEM
    steps = count // SEQ_STEP

    inner_window = jnp.swapaxes(inner_window, 0, 1)
    taps = inner_kernel.shape[0]
    inner = inner_weight.shape[1]
    mixer_args = [
        tokens,
        mixer_gain[None],
        gate_weight,
        inner_weight,
        state_weight,
        step_weight.T,
        step_bias[None],
        decay_log[None],
        skip_scale[None],
        inner_kernel,
        state_kernel,
        inner_window,
        state_window,
        recurrent_state,
        group_gain[None],
    ]
    held = [vmem(a.shape, a.dtype) for a in mixer_args]
    held[11] = vmem((taps,) + inner_window.shape[1:], bf16)
    held[12] = vmem((count, taps) + state_window.shape[2:], bf16)
    heads = step_bias.shape[0]
    n_state = state_weight.shape[2]
    mixer_rows, new_state, new_inner, new_state_window = pl.pallas_call(
        mixer,
        out_shape=[
            jax.ShapeDtypeStruct((count, inner), bf16),
            jax.ShapeDtypeStruct(recurrent_state.shape, f32),
            jax.ShapeDtypeStruct(inner_window.shape, bf16),
            jax.ShapeDtypeStruct(state_window.shape, bf16),
        ],
        in_specs=[hbm] * len(mixer_args),
        out_specs=[on_chip] + [hbm] * 3,
        scratch_shapes=held
        + [
            vmem((count, heads * n_state), f32),
            vmem((inner, 2 * count), f32),
            dma((14,)),
            dma((2, steps)),
            dma((2,)),
        ],
        compiler_params=pltpu.CompilerParams(vmem_limit_bytes=24 * 1024 * 1024),
    )(*[pltpu.with_memory_space_constraint(a, pltpu.HBM) for a in mixer_args])

    expert_gate = jnp.swapaxes(expert_gate, 1, 2)
    expert_up = jnp.swapaxes(expert_up, 1, 2)
    hidden_width = dense_gate.shape[1]
    expert_hidden = expert_gate.shape[1]
    slice_rows = hidden_width // tp_size
    if hidden_width % (8 * tp_size):
        slice_rows = hidden_width
    halves = tp_size // 2
    chunks = CHUNKS if ep_size == 8 else [(k, 8) for k in range(0, ep_size, 8)]
    live = max(length for _, length in chunks) * count
    wide = 2 * (expert_hidden + padded(slice_rows))
    branch_args = [
        mixer_rows,
        output_weight,
        tokens,
        channel_gain[None],
        routes.T,
        route_weights.T,
        dense_scale[None],
        expert_gate,
        expert_up,
        expert_down,
        dense_gate.T,
        dense_up.T,
        dense_down,
    ]
    new_tokens = pl.pallas_call(
        functools.partial(branches, ep_size, tp_size, slice_rows, chunks),
        out_shape=jax.ShapeDtypeStruct((count, own_width), bf16),
        in_specs=[on_chip] * 7 + [hbm] * (len(branch_args) - 7),
        out_specs=pl.BlockSpec(memory_space=pltpu.VMEM),
        scratch_shapes=[
            vmem((tp_size, 1, own_width), f32),
            vmem((wide, width), bf16),
            vmem(expert_down.shape[1:], bf16),
            vmem((tp_size, 3, slice_rows, own_width), bf16),
            vmem((ep_size, 1, LANES), f32),
            vmem((ep_size, 1, LANES), f32),
            vmem((2, halves, count, own_width), bf16),
            vmem((tp_size, halves, count, own_width), bf16),
            vmem((halves, count, own_width), f32),
            vmem((2, ep_size, halves, count, own_width), bf16),
            vmem((live, width), f32),
            vmem((wide, live), f32),
            vmem((live, expert_hidden), bf16),
            vmem((slice_rows, live), bf16),
            vmem((ep_size, count, own_width), f32),
            vmem((2, halves, ep_size, count, own_width), bf16),
            vmem((halves, ep_size, count, own_width), bf16),
            vmem((halves * ep_size, count, own_width), bf16),
            vmem((halves * ep_size, count, own_width), bf16),
            pltpu.SemaphoreType.REGULAR((3,)),
            dma((3,)),
            dma((2,)),
            dma((2,)),
            dma((2,)),
            dma((2,)),
            dma((1,)),
            dma((ep_size,)),
            dma((1,)),
            dma((ep_size,)),
            dma((2, halves * len(chunks))),
            dma((2,)),
        ],
        compiler_params=pltpu.CompilerParams(
            collective_id=0, has_side_effects=True, vmem_limit_bytes=(24 if ep_size <= 8 else 56) * 1024 * 1024
        ),
    )(*branch_args[:7], *[pltpu.with_memory_space_constraint(a, pltpu.HBM) for a in branch_args[7:]])
    return (
        new_tokens,
        new_state,
        jnp.swapaxes(new_inner, 0, 1),
        new_state_window,
    )


def solution(mesh):
    placed = (
        P("ep", None),
        P(),
        P(None, "tp"),
        P(None, "tp"),
        P(None, None, "tp"),
        P(None, "tp"),
        P("tp"),
        P("tp"),
        P("tp"),
        P(None, "tp"),
        P(None, None, "tp"),
        P("ep", None, "tp"),
        P("ep", None, None, "tp"),
        P("ep", "tp", None, None),
        P("tp"),
        P("tp", None),
        P(),
        P("ep", None),
        P("ep", None),
        P("ep", None, "tp"),
        P("ep", None, "tp"),
        P("ep", "tp", None),
        P("tp", "ep"),
        P("tp", "ep"),
        P("ep", "tp"),
        P("tp"),
    )
    return jax.shard_map(
        local,
        mesh=mesh,
        in_specs=placed,
        out_specs=(
            P("ep", "tp"),
            P("ep", "tp", None, None),
            P("ep", None, "tp"),
            P("ep", None, None, "tp"),
        ),
        check_vma=False,
    )
```

```python
import functools

import jax
import jax.numpy as jnp
from jax import lax
from jax.experimental import pallas as pl
from jax.experimental.pallas import tpu as pltpu
from jax.sharding import PartitionSpec as P

HEADS = 16
GROUPS = 4
HEAD_DIM = 64
STATE_DIM = 128
LANES = 128
SEQ_STEP = 6
DEST_ORDER = (0, 1, 7, 6, 5, 4, 3, 2)
CHUNKS = ((0, 8),)

eps = 1e-06


def silu(v):
    return v / (1.0 + jnp.exp(-v))


def dot_rows(rows, columns):
    return lax.dot_general(
        rows, columns, (((1,), (1,)), ((), ())), preferred_element_type=jnp.float32
    )


def dot(a, b):
    return jnp.dot(a, b, preferred_element_type=jnp.float32)


def mixer(
    tokens_hbm,
    mgain_hbm,
    gatew_hbm,
    innerw_hbm,
    statew_hbm,
    stepw_hbm,
    sbias_hbm,
    dlog_hbm,
    skip_hbm,
    ikern_hbm,
    skern_hbm,
    iwin_hbm,
    swin_hbm,
    state_hbm,
    ggain_hbm,
    rows_out,
    state_out,
    iwin_out,
    swin_out,
    tokens,
    mgain,
    gatew,
    innerw,
    statew,
    stepw,
    sbias,
    dlog,
    skip,
    ikern,
    skern,
    iwin,
    swin,
    state,
    ggain,
    decays,
    mixed,
    sems,
    state_sems,
    out_sems,
):
    f32 = jnp.float32
    bf16 = jnp.bfloat16
    count = tokens.shape[0]
    taps = ikern.shape[0]
    heads = sbias.shape[1]
    inner = innerw.shape[1]
    head_dim = inner // heads
    n_state = statew.shape[2]
    small = [
        (tokens_hbm, tokens),
        (mgain_hbm, mgain),
        (innerw_hbm, innerw),
        (statew_hbm, statew),
        (stepw_hbm, stepw),
        (sbias_hbm, sbias),
        (dlog_hbm, dlog),
        (ikern_hbm, ikern),
        (skern_hbm, skern),
        (iwin_hbm, iwin.at[pl.ds(0, taps - 1)]),
        (swin_hbm, swin.at[:, pl.ds(0, taps - 1)]),
        (gatew_hbm, gatew),
        (skip_hbm, skip),
        (ggain_hbm, ggain),
    ]
    loads = []
    for i, (src, dst) in enumerate(small):
        copy = pltpu.make_async_copy(src, dst, sems.at[i])
        if i < 11:
            copy.start()
        loads.append(copy)

    def state_load(i):
        at = pl.ds(i * SEQ_STEP, SEQ_STEP)
        return pltpu.make_async_copy(state_hbm.at[at], state.at[at], state_sems.at[0, i])

    def state_store(i):
        at = pl.ds(i * SEQ_STEP, SEQ_STEP)
        return pltpu.make_async_copy(state.at[at], state_out.at[at], state_sems.at[1, i])

    steps = count // SEQ_STEP
    loads[0].wait()
    loads[1].wait()
    for i in range(steps):
        state_load(i).start()
    for copy in loads[11:]:
        copy.start()
    value = tokens[...].astype(f32)
    squares = jnp.mean(value * value, axis=-1, keepdims=True)
    normed = (value * lax.rsqrt(squares + eps) * mgain[...]).astype(bf16)
    for i in range(2, 11):
        loads[i].wait()
    inner_pre = dot(normed, innerw[...]).astype(bf16)
    pre_u = dot(normed, statew[0])
    pre_c = dot(normed, statew[1])
    step_raw = dot_rows(normed, stepw[...])

    iwin[taps - 1] = inner_pre
    conv = inner_pre.astype(f32) * ikern[taps - 1 : taps, :]
    for j in range(taps - 1):
        conv = conv + iwin[j].astype(f32) * ikern[j : j + 1, :]
    inner_conv = silu(conv)

    both = jnp.concatenate([pre_u[:, None, :], pre_c[:, None, :]], axis=1).astype(bf16)
    swin[:, taps - 1] = both
    sconv = both.astype(f32) * skern[taps - 1][None]
    for j in range(taps - 1):
        sconv = sconv + swin[:, j].astype(f32) * skern[j][None]
    sconv = silu(sconv)
    u_vec = sconv[:, 0, :]
    c_vec = sconv[:, 1, :]
    win_copies = [
        pltpu.make_async_copy(iwin.at[pl.ds(1, taps - 1)], iwin_out, out_sems.at[0]),
        pltpu.make_async_copy(swin.at[:, pl.ds(1, taps - 1)], swin_out, out_sems.at[1]),
    ]
    for copy in win_copies:
        copy.start()

    step_size = jax.nn.softplus(step_raw + sbias[...])
    decay = jnp.exp(-step_size * jnp.exp(dlog[...]))
    step_wide = jnp.concatenate(
        [jnp.broadcast_to(step_size[:, h : h + 1], (count, head_dim)) for h in range(heads)],
        axis=1,
    )
    decay_wide = jnp.concatenate(
        [jnp.broadcast_to(decay[:, h : h + 1], (count, head_dim)) for h in range(heads)], axis=1
    )
    for h in range(heads):
        decays[:, h * n_state : (h + 1) * n_state] = jnp.broadcast_to(
            decay[:, h : h + 1], (count, n_state)
        )
    moved = step_wide * inner_conv
    written = moved.T.astype(bf16)
    row_of = lax.broadcasted_iota(jnp.int32, (count, n_state), 0)
    lane_of = lax.broadcasted_iota(jnp.int32, (inner, 2 * count), 1)
    none = jnp.zeros_like(c_vec)
    readers = jnp.concatenate(
        [jnp.concatenate([c_vec, none], axis=1), jnp.concatenate([none, c_vec], axis=1)], axis=0
    ).astype(bf16)

    for i in range(steps):
        state_load(i).wait()
        for b in range(i * SEQ_STEP, (i + 1) * SEQ_STEP, 2):
            pair = jnp.concatenate(
                [jnp.where(row_of == b + n, u_vec, 0.0) for n in range(2)], axis=1
            ).astype(bf16)
            outer = dot(written, pair)
            old = [
                jnp.concatenate([state[b + n, h].astype(bf16) for h in range(heads)], axis=0)
                for n in range(2)
            ]
            read = dot_rows(jnp.concatenate(old, axis=1), readers)
            if b:
                read = jnp.where((lane_of == b) | (lane_of == count + b + 1), read, mixed[...])
            mixed[...] = read
            for n in range(2):
                for h in range(heads):
                    fade = decays[b + n : b + n + 1, h * n_state : (h + 1) * n_state]
                    state[b + n, h] = (
                        state[b + n, h] * fade
                        + outer[h * head_dim : (h + 1) * head_dim, n * n_state : (n + 1) * n_state]
                    )
        state_store(i).start()

    for i in range(11, 14):
        loads[i].wait()
    gate_pre = dot(normed, gatew[...])
    read = mixed[...].T
    even = lax.rem(lax.broadcasted_iota(jnp.int32, (count, inner), 0), 2) == 0
    read = jnp.where(even, read[:count], read[count:])
    mixed_out = decay_wide * read + moved * jnp.sum(u_vec * c_vec, axis=1, keepdims=True)
    skip_wide = jnp.concatenate(
        [jnp.broadcast_to(skip[:, h : h + 1], (1, head_dim)) for h in range(heads)], axis=1
    )
    gated = (mixed_out + skip_wide * inner_conv) * silu(gate_pre)
    squares = jnp.mean(gated * gated, axis=-1, keepdims=True)
    rows_out[...] = (gated * lax.rsqrt(squares + eps) * ggain[...]).astype(bf16)
    for i in range(steps):
        state_store(i).wait()
    for copy in win_copies:
        copy.wait()


def padded(rows):
    return -(-rows // 16) * 16


def flipped(a, b):
    low = lax.rem(a + b, 2)
    high = lax.rem(a // 2 + b // 2, 2)
    return 2 * high + low


def flip(index, mask):
    moved = index
    bit = 1
    while bit <= mask:
        if mask & bit:
            moved = moved + bit * (1 - 2 * lax.rem(index // bit, 2))
        bit *= 2
    return moved


def branches(
    ep_size,
    tp_size,
    slice_rows,
    chunks,
    mrows,
    outw,
    tokens,
    gain,
    routes,
    rweights,
    scale,
    gate_hbm,
    up_hbm,
    down_hbm,
    dgate_hbm,
    dup_hbm,
    ddown_hbm,
    out,
    scales,
    weights_in,
    down_w,
    dense_w,
    table_send,
    tables,
    part,
    parts,
    residual,
    rows,
    flat,
    pre,
    act,
    hid,
    shares,
    y_part,
    y_recv,
    z_send,
    z_recv,
    near_sems,
    load_sems,
    part_sems,
    table_sems,
    scale_sems,
    dense_sems,
    row_send,
    row_sems,
    relay_send,
    relay_sems,
    y_sems,
    z_sems,
):
    f32 = jnp.float32
    bf16 = jnp.bfloat16
    me_e = lax.axis_index("ep")
    me_t = lax.axis_index("tp")
    side = me_t // 2
    core = lax.rem(me_t, 2)
    partner = flip(me_t, 1)
    count, width = tokens.shape
    own_width = width // tp_size
    hidden_width = dgate_hbm.shape[0]
    halves = tp_size // 2
    expert_hidden = gate_hbm.shape[1]
    dense_at = [2 * expert_hidden, 2 * expert_hidden + padded(slice_rows)]

    def remote(src, dst, send, recv, to_e, to_t):
        copy = pltpu.make_async_remote_copy(
            src_ref=src,
            dst_ref=dst,
            send_sem=send,
            recv_sem=recv,
            device_id=(to_e, to_t),
            device_id_type=pl.DeviceIdType.MESH,
        )
        copy.start()
        return copy

    def settle(ref, sem):
        pltpu.make_async_copy(ref, ref, sem).wait()

    def tell(sem, to_e, to_t):
        pl.semaphore_signal(
            sem, inc=1, device_id=(to_e, to_t), device_id_type=pl.DeviceIdType.MESH
        )

    barrier = pltpu.get_barrier_semaphore()
    staged = ep_size == 8
    line = me_e // 2
    last = ep_size // 2 - 1

    def tell_line(sem, distance, to_t):
        pl.when(line >= distance)(lambda: tell(sem, me_e - 2 * distance, to_t))
        pl.when(line + distance <= last)(lambda: tell(sem, me_e + 2 * distance, to_t))

    def line_peers(distance):
        below = jnp.where(line >= distance, 1, 0)
        return below + jnp.where(line + distance <= last, 1, 0)

    for m in range(1, tp_size):
        tell(barrier, me_e, flip(me_t, m))
    if staged:
        tell(barrier, flip(me_e, 1), me_t)
        tell_line(barrier, 1, me_t)
    else:
        for m in range(ep_size - 1, 0, -1):
            tell(barrier, flip(me_e, m), partner)

    def dense_rows(ref, t):
        if slice_rows == hidden_width:
            return ref
        return ref.at[pl.ds(t * slice_rows, slice_rows)]

    dense_hbm = [dgate_hbm, dup_hbm, ddown_hbm]
    for src, dst, sem in [
        (gate_hbm.at[0], weights_in.at[pl.ds(0, expert_hidden)], 0),
        (up_hbm.at[0], weights_in.at[pl.ds(expert_hidden, expert_hidden)], 0),
        (down_hbm.at[0], down_w, 1),
    ] + [(dense_rows(dense_hbm[k], me_t), dense_w.at[0, k], 2) for k in range(3)]:
        pltpu.make_async_copy(src, dst, load_sems.at[sem]).start()

    mixer_rows = mrows[...]
    for q in range(tp_size):
        piece = dot(mixer_rows, outw[:, q * own_width : (q + 1) * own_width])
        part[q % 2, q // 2] = piece.astype(bf16)
    scales[0] = scale[...]

    if staged:
        pl.semaphore_wait(barrier, tp_size + line_peers(1))
        tell_line(near_sems.at[0], 1, me_t)
    else:
        pl.semaphore_wait(barrier, ep_size + tp_size - 2)
    tp_order = [m for m in range(2, tp_size)] + [1]
    for m in tp_order:
        to = flip(me_t, m)
        remote(
            part.at[lax.rem(to, 2)], parts.at[m], part_sems.at[0], part_sems.at[1], me_e, to
        )
    for m in tp_order:
        to = flip(me_t, m)
        remote(scales.at[0], scales.at[m], scale_sems.at[0], scale_sems.at[1], me_e, to)
        for k in range(3):
            remote(
                dense_rows(dense_hbm[k], to),
                dense_w.at[m, k],
                dense_sems.at[0],
                dense_sems.at[1],
                me_e,
                to,
            )

    expert_of = lax.broadcasted_iota(jnp.int32, (ep_size, count), 0)
    table = jnp.zeros((ep_size, count), f32)
    for k in range(routes.shape[0]):
        table = table + jnp.where(expert_of == routes[k : k + 1, :], rweights[k : k + 1, :], 0.0)
    table = jnp.concatenate([table, jnp.zeros((ep_size, LANES - count), f32)], axis=1)
    for m in range(ep_size):
        table_send[m] = table[m : m + 1]
    tables[me_e] = table_send[me_e]
    if staged:
        pl.semaphore_wait(near_sems.at[0], line_peers(1))
        tell_line(near_sems.at[1], 1, me_t)
        tell_line(near_sems.at[1], 2, me_t)
        pl.semaphore_wait(near_sems.at[1], line_peers(1) + line_peers(2))
        tell(near_sems.at[2], me_e, partner)
    own_rows = []
    for h in range(halves):
        at = pl.ds(pl.multiple_of(core * own_width + 2 * h * own_width, own_width), own_width)
        own_rows.append(tokens[:, at].astype(f32) + part[core, h].astype(f32))
    settle(parts.at[pl.ds(1, tp_size - 1)], part_sems.at[1])
    for h in range(halves):
        for m in range(1, tp_size):
            own_rows[h] = own_rows[h] + parts[m, h].astype(f32)
        residual[h] = own_rows[h]
        rows[core, me_e, h] = own_rows[h].astype(bf16)

    if staged:
        pl.semaphore_wait(near_sems.at[2], 1)
    for m in range(ep_size - 1, 0, -1):
        remote(
            rows.at[core, me_e],
            rows.at[core, me_e],
            row_send.at[0],
            row_sems.at[me_e],
            flip(me_e, m),
            partner,
        )
    for m in range(1, ep_size):
        remote(
            table_send.at[flip(me_e, m)],
            tables.at[me_e],
            table_sems.at[0],
            table_sems.at[1],
            flip(me_e, m),
            partner,
        )

    def block_of(chunk, place):
        start, length = chunk
        return start + flip(lax.rem(me_e, length), place)

    def is_home(chunk):
        start, length = chunk
        return me_e // length == start // length

    def relay(chunk, place):
        m = block_of(chunk, place)

        def pass_on(half):
            remote(
                rows.at[half, m],
                rows.at[half, m],
                relay_send.at[0],
                relay_sems.at[chunk[0] // chunk[1]],
                me_e,
                partner,
            )

        def forward():
            settle(rows.at[1 - core, m], row_sems.at[m])
            pass_on(1 - core)

        if place:
            forward()
        else:
            home = is_home(chunk)
            pl.when(home)(lambda: pass_on(core))
            pl.when(jnp.logical_not(home))(forward)

    def normalize(chunk, places):
        blocks = [(at, block_of(chunk, at)) for at in places]
        sem = relay_sems.at[chunk[0] // chunk[1]]
        settle(rows.at[0, pl.ds(chunk[0], chunk[1])], sem)
        for at, m in blocks:
            pieces = [rows[q % 2, m, q // 2].astype(f32) for q in range(tp_size)]
            squares = pieces[0] * pieces[0]
            for q in range(1, tp_size):
                squares = squares + pieces[q] * pieces[q]
            scale_of = lax.rsqrt(jnp.sum(squares, axis=-1, keepdims=True) * (1.0 / width) + eps)
            for q in range(tp_size):
                lanes = slice(q * own_width, (q + 1) * own_width)
                flat[at * count : (at + 1) * count, lanes] = pieces[q] * scale_of * gain[:, lanes]

    unit = LANES
    if slice_rows == hidden_width:
        units = lax.broadcasted_iota(jnp.int32, (slice_rows, 1), 0)
        share = hidden_width // tp_size
        kept = (units // share == me_t).astype(f32)

    def weigh(m):
        row = tables[m][:, :count]
        diagonal = lax.broadcasted_iota(jnp.int32, (count, count), 0) == lax.broadcasted_iota(
            jnp.int32, (count, count), 1
        )
        weight = jnp.sum(jnp.where(diagonal, row, 0.0), axis=1, keepdims=True)
        shares[m] = jnp.broadcast_to(weight, (count, own_width))

    def place_weights():
        settle(weights_in.at[pl.ds(0, 2 * expert_hidden)], load_sems.at[0])
        settle(down_w, load_sems.at[1])
        settle(dense_w.at[0], load_sems.at[2])
        settle(tables.at[pl.ds(0, ep_size - 1)], table_sems.at[1])
        settle(scales.at[pl.ds(1, tp_size - 1)], scale_sems.at[1])
        settle(dense_w.at[pl.ds(1, tp_size - 1)], dense_sems.at[1])
        for k in range(2):
            at = slice(dense_at[k], dense_at[k] + slice_rows)
            for m in range(tp_size):
                lanes = pl.ds(pl.multiple_of(flip(me_t, m) * own_width, own_width), own_width)
                weights_in[at, lanes] = dense_w[m, k]
        for m in range(ep_size):
            weigh(m)

    def activate(chunk):
        live = chunk[1] * count
        lanes = slice(0, live)
        x = flat[:live, :].astype(bf16)
        pre[:, lanes] = dot_rows(weights_in[...], x)
        for n in range(0, expert_hidden, unit):
            end = min(n + unit, expert_hidden)
            gate_act = pre[n:end, lanes]
            up_act = pre[expert_hidden + n : expert_hidden + end, lanes]
            act[lanes, n:end] = (silu(gate_act) * up_act).T.astype(bf16)
        gate_act = pre[dense_at[0] : dense_at[0] + slice_rows, lanes]
        up_act = pre[dense_at[1] : dense_at[1] + slice_rows, lanes]
        hidden = silu(gate_act) * up_act
        if slice_rows == hidden_width:
            hidden = hidden * kept
        hid[:, lanes] = hidden.astype(bf16)

    contract_rows = (((0,), (0,)), ((), ()))

    def project(chunk, first):
        live = chunk[1] * count
        weights = [shares[block_of(chunk, g)] for g in range(chunk[1])]
        acts = act[:live, :]
        hidden = hid[:, :live]
        for mine in range(2):
            whose = 1 - core if mine else core
            for h in range(halves):
                t = 2 * h + whose
                lanes = pl.ds(pl.multiple_of(t * own_width, own_width), own_width)
                slot = flipped(me_t, t)
                routed = dot(acts, down_w[:, lanes])
                dense = lax.dot_general(
                    hidden, dense_w[slot, 2], contract_rows, preferred_element_type=f32
                )
                for g in range(chunk[1]):
                    at = slice(g * count, (g + 1) * count)
                    y = routed[at] * weights[g] + dense[at] * scales[slot]
                    y_part[mine, h, first + g] = y.astype(bf16)
                if not mine:
                    at = pl.ds(first, chunk[1])
                    y_copies.append(
                        remote(
                            y_part.at[0, h, at],
                            y_recv.at[h, at],
                            y_sems.at[0, len(y_copies)],
                            y_sems.at[1, len(y_copies)],
                            me_e,
                            partner,
                        )
                    )
    def give_back(chunk, first, sent):
        for to_side in range(halves):
            sent[to_side].wait_recv()
            for n in range(chunk[1]):
                if ep_size == 8:
                    m = DEST_ORDER[n]
                    place = flip(me_e, m)
                else:
                    place = first + chunk[1] - 1 - n
                    m = block_of(chunk, chunk[1] - 1 - n)
                at = to_side * ep_size + place
                summed = y_part[1, to_side, place].astype(f32)
                summed = summed + y_recv[to_side, place].astype(f32)
                z_send[at] = summed.astype(bf16)
                remote(
                    z_send.at[at],
                    z_recv.at[side * ep_size + me_e],
                    z_sems.at[0],
                    z_sems.at[1],
                    m,
                    2 * to_side + 1 - core,
                )

    y_copies = []
    for k, chunk in enumerate(chunks):
        for place in range(chunk[1]):
            relay(chunk, place)
        if k == 0:
            place_weights()
        normalize(chunk, range(chunk[1]))
        activate(chunk)
        project(chunk, chunk[0])
        give_back(chunk, chunk[0], y_copies[halves * k :])

    settle(z_recv, z_sems.at[1])
    final = residual[side]
    for m in range(halves * ep_size):
        final = final + z_recv[m].astype(f32)
    out[...] = final.astype(bf16)

    settle(parts.at[pl.ds(1, tp_size - 1)], part_sems.at[0])
    settle(tables.at[pl.ds(0, ep_size - 1)], table_sems.at[0])
    settle(scales.at[pl.ds(1, tp_size - 1)], scale_sems.at[0])
    settle(dense_w.at[pl.ds(1, tp_size - 1)], dense_sems.at[0])
    settle(rows.at[0, pl.ds(1, ep_size - 1)], row_send.at[0])
    settle(rows.at[0], relay_send.at[0])
    for copy in y_copies:
        copy.wait_send()
    settle(z_send, z_sems.at[0])


def local(
    tokens,
    mixer_gain,
    gate_weight,
    inner_weight,
    state_weight,
    step_weight,
    step_bias,
    decay_log,
    skip_scale,
    inner_kernel,
    state_kernel,
    inner_window,
    state_window,
    recurrent_state,
    group_gain,
    output_weight,
    channel_gain,
    routes,
    route_weights,
    expert_gate,
    expert_up,
    expert_down,
    dense_gate,
    dense_up,
    dense_down,
    dense_scale,
):
    f32 = jnp.float32
    bf16 = jnp.bfloat16
    ep_size = lax.axis_size("ep")
    tp_size = lax.axis_size("tp")
    count, width = tokens.shape
    own_width = width // tp_size
    hbm = pl.BlockSpec(memory_space=pltpu.HBM)
    on_chip = pl.BlockSpec(memory_space=pltpu.VMEM)
    dma = pltpu.SemaphoreType.DMA
    vmem = pltpu.VMEM
    steps = count // SEQ_STEP

    inner_window = jnp.swapaxes(inner_window, 0, 1)
    taps = inner_kernel.shape[0]
    inner = inner_weight.shape[1]
    mixer_args = [
        tokens,
        mixer_gain[None],
        gate_weight,
        inner_weight,
        state_weight,
        step_weight.T,
        step_bias[None],
        decay_log[None],
        skip_scale[None],
        inner_kernel,
        state_kernel,
        inner_window,
        state_window,
        recurrent_state,
        group_gain[None],
    ]
    held = [vmem(a.shape, a.dtype) for a in mixer_args]
    held[11] = vmem((taps,) + inner_window.shape[1:], bf16)
    held[12] = vmem((count, taps) + state_window.shape[2:], bf16)
    heads = step_bias.shape[0]
    n_state = state_weight.shape[2]
    mixer_rows, new_state, new_inner, new_state_window = pl.pallas_call(
        mixer,
        out_shape=[
            jax.ShapeDtypeStruct((count, inner), bf16),
            jax.ShapeDtypeStruct(recurrent_state.shape, f32),
            jax.ShapeDtypeStruct(inner_window.shape, bf16),
            jax.ShapeDtypeStruct(state_window.shape, bf16),
        ],
        in_specs=[hbm] * len(mixer_args),
        out_specs=[on_chip] + [hbm] * 3,
        scratch_shapes=held
        + [
            vmem((count, heads * n_state), f32),
            vmem((inner, 2 * count), f32),
            dma((14,)),
            dma((2, steps)),
            dma((2,)),
        ],
        compiler_params=pltpu.CompilerParams(vmem_limit_bytes=24 * 1024 * 1024),
    )(*[pltpu.with_memory_space_constraint(a, pltpu.HBM) for a in mixer_args])

    expert_gate = jnp.swapaxes(expert_gate, 1, 2)
    expert_up = jnp.swapaxes(expert_up, 1, 2)
    hidden_width = dense_gate.shape[1]
    expert_hidden = expert_gate.shape[1]
    slice_rows = hidden_width // tp_size
    if hidden_width % (8 * tp_size):
        slice_rows = hidden_width
    halves = tp_size // 2
    chunks = CHUNKS if ep_size == 8 else [(k, 8) for k in range(0, ep_size, 8)]
    live = max(length for _, length in chunks) * count
    wide = 2 * (expert_hidden + padded(slice_rows))
    branch_args = [
        mixer_rows,
        output_weight,
        tokens,
        channel_gain[None],
        routes.T,
        route_weights.T,
        dense_scale[None],
        expert_gate,
        expert_up,
        expert_down,
        dense_gate.T,
        dense_up.T,
        dense_down,
    ]
    new_tokens = pl.pallas_call(
        functools.partial(branches, ep_size, tp_size, slice_rows, chunks),
        out_shape=jax.ShapeDtypeStruct((count, own_width), bf16),
        in_specs=[on_chip] * 7 + [hbm] * (len(branch_args) - 7),
        out_specs=pl.BlockSpec(memory_space=pltpu.VMEM),
        scratch_shapes=[
            vmem((tp_size, 1, own_width), f32),
            vmem((wide, width), bf16),
            vmem(expert_down.shape[1:], bf16),
            vmem((tp_size, 3, slice_rows, own_width), bf16),
            vmem((ep_size, 1, LANES), f32),
            vmem((ep_size, 1, LANES), f32),
            vmem((2, halves, count, own_width), bf16),
            vmem((tp_size, halves, count, own_width), bf16),
            vmem((halves, count, own_width), f32),
            vmem((2, ep_size, halves, count, own_width), bf16),
            vmem((live, width), f32),
            vmem((wide, live), f32),
            vmem((live, expert_hidden), bf16),
            vmem((slice_rows, live), bf16),
            vmem((ep_size, count, own_width), f32),
            vmem((2, halves, ep_size, count, own_width), bf16),
            vmem((halves, ep_size, count, own_width), bf16),
            vmem((halves * ep_size, count, own_width), bf16),
            vmem((halves * ep_size, count, own_width), bf16),
            pltpu.SemaphoreType.REGULAR((3,)),
            dma((3,)),
            dma((2,)),
            dma((2,)),
            dma((2,)),
            dma((2,)),
            dma((1,)),
            dma((ep_size,)),
            dma((1,)),
            dma((len(chunks),)),
            dma((2, halves * len(chunks))),
            dma((2,)),
        ],
        compiler_params=pltpu.CompilerParams(
            collective_id=0, has_side_effects=True, vmem_limit_bytes=(24 if ep_size <= 8 else 56) * 1024 * 1024
        ),
    )(*branch_args[:7], *[pltpu.with_memory_space_constraint(a, pltpu.HBM) for a in branch_args[7:]])
    return (
        new_tokens,
        new_state,
        jnp.swapaxes(new_inner, 0, 1),
        new_state_window,
    )


def solution(mesh):
    placed = (
        P("ep", None),
        P(),
        P(None, "tp"),
        P(None, "tp"),
        P(None, None, "tp"),
        P(None, "tp"),
        P("tp"),
        P("tp"),
        P("tp"),
        P(None, "tp"),
        P(None, None, "tp"),
        P("ep", None, "tp"),
        P("ep", None, None, "tp"),
        P("ep", "tp", None, None),
        P("tp"),
        P("tp", None),
        P(),
        P("ep", None),
        P("ep", None),
        P("ep", None, "tp"),
        P("ep", None, "tp"),
        P("ep", "tp", None),
        P("tp", "ep"),
        P("tp", "ep"),
        P("ep", "tp"),
        P("tp"),
    )
    return jax.shard_map(
        local,
        mesh=mesh,
        in_specs=placed,
        out_specs=(
            P("ep", "tp"),
            P("ep", "tp", None, None),
            P("ep", None, "tp"),
            P("ep", None, None, "tp"),
        ),
        check_vma=False,
    )
```
